256 devices in a mesh: sp: 64 (over z, y, core), tp: 4 (over x).
Axes of the slice: x: 4, y: 4, z: 8, core: 2. Of those that a mesh axis runs over, the one named last changes fastest.
Arguments:
- tokens: bfloat16 [10240, 2048], P('sp'), may hold values from -8 to 8
- query_weight: bfloat16 [2048, 2048], P('sp', 'tp'), may hold values from -0.5 to 0.5
- key_weight: bfloat16 [2048, 2048], P('sp', 'tp'), may hold values from -0.5 to 0.5
- value_weight: bfloat16 [2048, 2048], P('sp', 'tp'), may hold values from -0.125 to 0.125
- out_weight: bfloat16 [2048, 2048], P('tp', 'sp'), may hold values from -0.125 to 0.125
- mix_lambda: float32 [16], P('tp'), may hold values from 0.3 to 0.8
- head_gain: float32 [128], replicated, may hold values from 0.1 to 1.9
Outputs:
- attended: bfloat16 [10240, 2048], P('sp')
The draws below stay inside these ranges and needn't reach their ends.
All inputs are finite; a program needn't handle non-finite values.
Results may differ from the reference program's by a relative error of at most 0.018.
The reference program's roundings to bfloat16 on the way (of `queries`, `keys`, `values` and `head_out`) count: a program that leaves them out, or rounds other values in their place, can miss the bound.
Values may be sent and summed in bfloat16 or wider, within the bound.
A program may use at most 192 MiB of HBM per device.

```python
import math
import jax
import jax.numpy as jnp
from jax import lax

D = 2048
HEADS = 16
QKD = 64
VDIM = 128
TOK_DEV = 160
SEQ = 10240


def draw_tokens(key, part):
    noise_key, mean_key = jax.random.split(key, 2)
    block_count = SEQ // TOK_DEV
    base = jnp.clip(jax.random.normal(noise_key, (SEQ, D), jnp.float32), -4.0, 4.0)
    offsets = jnp.clip(0.7 * jax.random.normal(mean_key, (block_count, D), jnp.float32), -2.0, 2.0)
    drawn = base + jnp.repeat(offsets, TOK_DEV, axis=0)
    return drawn.astype(jnp.bfloat16)


def projection_draw(key, salt):
    spread = (D * 6 // 7) ** (-0.5)
    noise = spread * jax.random.normal(jax.random.fold_in(key, salt), (D, HEADS * 2 * QKD), jnp.float32)
    drawn = jnp.clip(noise, -0.5, 0.5)
    return drawn.astype(jnp.bfloat16)


def draw_query_weight(key, part):
    return projection_draw(key, 101)


def draw_key_weight(key, part):
    return projection_draw(key, 202)


def block_levels(own_key, shape, pieces, low, high):
    loudness = 1.0
    for axis_at, shards_of in pieces:
        steps = jax.random.uniform(jax.random.fold_in(jax.random.fold_in(own_key, 6), axis_at), (shards_of,), jnp.float32, low / len(pieces), high / len(pieces))
        loudness = loudness * jnp.repeat(jnp.exp(steps), shape[axis_at] // shards_of).reshape((-1,) + (1,) * (len(shape) - 1 - axis_at))
    return loudness


def normal_values(key, shape, scale, most, shards=(), kind=jnp.bfloat16):
    entries = jax.random.normal(key, shape, jnp.float32) * scale
    if len(shards) > 0:
        entries = block_levels(key, shape, shards, -0.22, 0.18) * entries
    return jnp.clip(entries, min=-most, max=most).astype(kind)


def setup_inputs(seed: int = 0) -> dict:
    splits = jax.random.split(jax.random.key(seed), 8)
    return {
        "tokens": draw_tokens(jax.random.fold_in(splits[7], 71), 0),
        "query_weight": draw_query_weight(jax.random.fold_in(splits[7], 71), 0),
        "key_weight": draw_key_weight(jax.random.fold_in(splits[7], 71), 0),
        "value_weight": normal_values(splits[3], (D, HEADS * VDIM), D ** -0.5, 0.125, ((0, 64), (1, 4))),
        "out_weight": normal_values(splits[4], (HEADS * VDIM, D), (HEADS * VDIM) ** -0.5, 0.125, ((0, 4), (1, 64))),
        "mix_lambda": jnp.clip(0.3 + 0.5 * jax.random.uniform(splits[5], (HEADS,), jnp.float32) ** block_levels(splits[5], (HEADS,), ((0, 4),), -0.2, 0.2), 0.3, 0.8),
        "head_gain": jnp.clip(1.0 + 0.18 * jax.random.normal(splits[6], (VDIM,), jnp.float32), 0.1, 1.9),
    }


def reference(tokens, query_weight, key_weight, value_weight, out_weight, mix_lambda, head_gain):
    length = tokens.shape[0]
    queries = jnp.dot(tokens, query_weight, preferred_element_type=jnp.float32).astype(jnp.bfloat16)
    keys = jnp.dot(tokens, key_weight, preferred_element_type=jnp.float32).astype(jnp.bfloat16)
    values = jnp.dot(tokens, value_weight, preferred_element_type=jnp.float32).astype(jnp.bfloat16)
    queries = queries.reshape(length, HEADS, 2, QKD)
    keys32 = keys.reshape(length, HEADS, 2, QKD).astype(jnp.float32)
    values32 = values.reshape(length, HEADS, VDIM).astype(jnp.float32)
    block_size = math.gcd(length, 512)
    block_count = length // block_size
    score_scale = QKD ** (-0.5)
    key_pos = jnp.arange(length, dtype=jnp.int32)

    def one_block(block_index):
        first_row = (block_index * block_size).astype(jnp.int32)
        query_rows = lax.dynamic_slice_in_dim(queries, first_row, block_size, 0).astype(jnp.float32)
        scores = jnp.einsum('qhcd,khcd->hcqk', query_rows, keys32) * score_scale
        query_pos = first_row + jnp.arange(block_size, dtype=jnp.int32)
        visible = key_pos[None, :] <= query_pos[:, None]
        scores = jnp.where(visible, scores, -jnp.inf)
        probabilities = jax.nn.softmax(scores, axis=-1)
        weights = probabilities[:, 0] - mix_lambda[:, None, None] * probabilities[:, 1]
        mixture = jnp.einsum('hqk,khd->qhd', weights, values32)
        normalized = mixture * lax.rsqrt(lax.optimization_barrier(jnp.mean(mixture * mixture, axis=-1, keepdims=True)) + 1e-05) * head_gain
        return normalized.astype(jnp.bfloat16)
    head_out = lax.map(one_block, jnp.arange(block_count, dtype=jnp.int32))
    head_out = head_out.reshape(length, HEADS * VDIM)
    return jnp.dot(head_out, out_weight, preferred_element_type=jnp.float32).astype(jnp.bfloat16)
```

```python
import functools
import math

import jax
import jax.numpy as jnp
from jax import lax
from jax.experimental import pallas as pl
from jax.experimental.pallas import tpu as pltpu
from jax.sharding import Mesh
from jax.sharding import PartitionSpec as P

MESH = pl.DeviceIdType.MESH
NZ, NY, NC, NX = 8, 4, 2, 4
ROWS = 160
TOKS = NY * ROWS
HEAD = 128
COLS = 2 * TOKS
TILE = 256
LOW = -1e30
EXP_SCALE = 64 ** (-0.5) * math.log2(math.e)


def rcopy(src, dst, send_sem, recv_sem, device):
    return pltpu.make_async_remote_copy(
        src_ref=src, dst_ref=dst, send_sem=send_sem, recv_sem=recv_sem, device_id=device, device_id_type=MESH
    )


class ZRing:
    def __init__(self, block, send, recv, sib_send):
        self.block, self.send, self.recv, self.sib_send = block, send, recv, sib_send
        self.z, self.c = lax.axis_index("z"), lax.axis_index("core")

    def origin(self, way, d):
        return lax.rem(self.z + (NZ - d if way == 0 else d), NZ)

    def farthest(self, way, kind):
        return NZ // 2 - (way != kind)

    def onward(self, way, d, kind, o):
        ref = self.block(o, self.c, kind)
        to = lax.rem(self.z + (1 if way == 0 else NZ - 1), NZ)
        return rcopy(ref, ref, self.send.at[way, d - 1, kind], self.recv.at[o, self.c, kind], {"z": to})

    def share(self, o, kind):
        ref = self.block(o, self.c, kind)
        return rcopy(ref, ref, self.sib_send.at[o, kind], self.recv.at[o, self.c, kind], {"core": 1 - self.c})

    def arrived(self, o, c, kind):
        ref = self.block(o, c, kind)
        rcopy(ref, ref, self.sib_send.at[o, kind], self.recv.at[o, c, kind], {"core": 1 - self.c}).wait_recv()

    def begin(self, kind):
        for way in (0, 1):
            self.onward(way, 1, kind, self.z).start()
        self.share(self.z, kind).start()

    def pass_on(self, way, d, kind):
        o = self.origin(way, d)
        self.arrived(o, self.c, kind)

        @pl.when(d < self.farthest(way, kind))
        def _():
            self.onward(way, d + 1, kind, o).start()

        self.share(o, kind).start()

    def drain(self):
        for kind in (0, 1):
            for way in (0, 1):
                for d in range(1, self.farthest(way, kind) + 1):
                    self.onward(way, d, kind, self.z).wait_send()

            @pl.loop(0, NZ)
            def _(o):
                self.share(o, kind).wait_send()


def attention_kernel(
    tok, wq, wk, wv, lam, gain, out,
    xbuf, wbuf, kbuf, vbuf, qrow, vrow, qbd, acc, top,
    tok_s, tok_r, wy_s, wy_r, w_s, w_r, w_sib, kv_s, kv_r, kv_sib,
):
    z, y, c = lax.axis_index("z"), lax.axis_index("y"), lax.axis_index("core")
    above, below = lax.rem(y + 1, NY), lax.rem(y + NY - 1, NY)
    across = lax.rem(y + 2, NY)

    barrier = pltpu.get_barrier_semaphore()
    friends = [{"y": lax.rem(y + k, NY)} for k in range(1, NY)]
    friends += [{"z": lax.rem(z + 1, NZ)}, {"z": lax.rem(z + NZ - 1, NZ)}, {"core": 1 - c}]
    for friend in friends:
        pl.semaphore_signal(barrier, inc=1, device_id=friend, device_id_type=MESH)
    pl.semaphore_wait(barrier, len(friends))

    half = ROWS // 2

    def part(slot, k):
        return xbuf.at[slot, pl.ds(k * half, half), :]

    def tok_copy(src, slot, k, n, to):
        return rcopy(src, part(slot, k), tok_s.at[n], tok_r.at[slot, k], {"y": to})

    def tok_arrived(slot, k):
        tok_copy(part(slot, k), slot, k, 0, above).wait_recv()

    def w_copy(to, k, n):
        src = (wq, wk, wv)[n].at[:, pl.ds(pl.multiple_of(to * HEAD, HEAD), HEAD)]
        dst = wbuf.at[z, y, c, :, pl.ds(n * HEAD, HEAD)]
        return rcopy(src, dst, wy_s.at[k, n], wy_r.at[y, n], {"y": to})

    for k in range(1, NY):
        for n in range(3):
            w_copy(lax.rem(y + k, NY), k - 1, n).start()
    own = [
        tok_copy(tok.at[pl.ds(0, half), :], y, 0, 0, above),
        tok_copy(tok.at[pl.ds(half, half), :], y, 1, 1, below),
        tok_copy(tok.at[pl.ds(half, half), :], y, 1, 2, above),
        tok_copy(tok.at[pl.ds(0, half), :], y, 0, 3, below),
    ]
    for copy in own:
        copy.start()

    mine = pl.ds(pl.multiple_of(y * HEAD, HEAD), HEAD)
    for n, w in enumerate((wq, wk, wv)):
        wbuf[z, y, c, :, n * HEAD : (n + 1) * HEAD] = w[:, mine]
    xbuf[y] = tok[...]
    acc[...] = jnp.zeros_like(acc)
    top[...] = jnp.full_like(top, LOW)

    for k in range(1, NY):
        frm = lax.rem(y + k, NY)
        for n in range(3):
            dst = wbuf.at[z, frm, c, :, pl.ds(n * HEAD, HEAD)]
            rcopy(dst, dst, wy_s.at[k - 1, n], wy_r.at[frm, n], {"y": frm}).wait_recv()

    wring = ZRing(lambda o, cc, kind: wbuf.at[o, pl.ds(2 * kind, 2), cc], w_s, w_r, w_sib)
    for kind in (0, 1):
        wring.begin(kind)
    fwd_up = tok_copy(part(below, 0), below, 0, 4, above)
    fwd_down = tok_copy(part(above, 1), above, 1, 5, below)
    for d in range(1, NZ // 2 + 1):
        for kind in (0, 1):
            for way in (0, 1):
                if d <= wring.farthest(way, kind):
                    wring.pass_on(way, d, kind)
        if d == 2:
            tok_arrived(below, 0)
            fwd_up.start()
            tok_arrived(above, 1)
            fwd_down.start()
    for o in range(NZ):
        for kind in (0, 1):
            wring.arrived(o, 1 - c, kind)

    def project(i, carry):
        away = jnp.where(i == 2, 3, jnp.where(i == 3, 2, i))
        slot = lax.rem(y + away, NY)

        @pl.when(i == 1)
        def _():
            tok_arrived(above, 0)

        @pl.when(i == 2)
        def _():
            tok_arrived(below, 1)

        @pl.when(i == 3)
        def _():
            tok_arrived(across, 0)
            tok_arrived(across, 1)

        made = jnp.dot(
            xbuf[slot], wbuf[...].reshape(-1, 3 * HEAD), preferred_element_type=jnp.float32
        ).astype(jnp.bfloat16)
        at = pl.ds(pl.multiple_of(slot * ROWS, ROWS), ROWS)
        qrow[at, :] = made[:, :HEAD]
        kbuf[z, c, at, :] = made[:, HEAD : 2 * HEAD]
        vrow[at, :] = made[:, 2 * HEAD :]
        return carry

    lax.fori_loop(0, NY, project, 0)
    vbuf[z, c] = vrow[...].T

    ring = ZRing(lambda o, cc, kind: (kbuf, vbuf)[kind].at[o, cc], kv_s, kv_r, kv_sib)
    for kind in (0, 1):
        ring.begin(kind)

    q_t = qrow[...].T
    first = lax.broadcasted_iota(jnp.int32, q_t.shape, 0) < HEAD // 2
    zero = jnp.zeros_like(q_t)
    qbd[:, :TOKS] = jnp.where(first, q_t, zero)
    qbd[:, TOKS:] = jnp.where(first, zero, q_t)

    ones = jnp.ones((16, TOKS), jnp.bfloat16)

    def visit(o, cc, masked):
        keys = kbuf[o, cc]
        values = jnp.concatenate([vbuf[o, cc], ones], axis=0)
        for j in range(COLS // TILE):
            cols = slice(j * TILE, (j + 1) * TILE)
            s = jnp.dot(keys, qbd[:, cols], preferred_element_type=jnp.float32)
            if masked:
                u = lax.broadcasted_iota(jnp.int32, (TOKS, 1), 0)
                t = lax.broadcasted_iota(jnp.int32, (1, TILE), 1) + j * TILE
                t = jnp.where(t >= TOKS, t - TOKS, t)

                def place(r, core):
                    skipped = sum((r >= k * ROWS).astype(jnp.int32) for k in range(1, NY))
                    return r + ROWS * (skipped + core)

                s = jnp.where(place(u, cc) <= place(t, c), s, LOW)
            before = top[0:1, cols]
            now = jnp.maximum(before, jnp.max(s, axis=0, keepdims=True))
            shrink = jnp.exp2((before - now) * EXP_SCALE)
            p = jnp.exp2((s - now) * EXP_SCALE).astype(jnp.bfloat16)
            acc[:, cols] = acc[:, cols] * shrink + jnp.dot(values, p, preferred_element_type=jnp.float32)
            top[0:1, cols] = now

    def own_slice(k, carry):
        cc = jnp.where(k == 0, c, 1 - c)

        @pl.when(k == 1)
        def _():
            for kind in (0, 1):
                ring.arrived(z, 1 - c, kind)

        visit(z, cc, True)
        return carry

    lax.fori_loop(0, NC, own_slice, 0)

    def step(d, carry):
        for kind in (0, 1):
            for way in (0, 1):
                @pl.when(d <= ring.farthest(way, kind))
                def _():
                    ring.pass_on(way, d, kind)

            way = kind
            before = d - 1
            o = ring.origin(way, before)
            there = (before >= 1) & (before <= NZ // 2 - way)

            @pl.when(there)
            def _():
                for other in (0, 1):
                    ring.arrived(o, 1 - c, other)

            @pl.when(there & (o < z))
            def _():
                def both(cc, carry):
                    visit(o, cc, False)
                    return carry

                lax.fori_loop(0, NC, both, 0)

        return carry

    lax.fori_loop(1, NZ // 2 + 2, step, 0)

    def part_of(cols):
        return acc[:HEAD, cols] / acc[HEAD : HEAD + 1, cols]

    mixture = part_of(slice(0, TOKS)) - lam[y] * part_of(slice(TOKS, COLS))
    scale = lax.rsqrt(jnp.mean(mixture * mixture, axis=0, keepdims=True) + 1e-05)
    out[...] = (mixture * scale * gain[...]).T.astype(jnp.bfloat16)

    for copy in own + [fwd_up, fwd_down]:
        copy.wait_send()
    for k in range(1, NY):
        for n in range(3):
            w_copy(lax.rem(y + k, NY), k - 1, n).wait_send()
    wring.drain()
    ring.drain()


def attention(tokens, wq, wk, wv, lam, gain):
    vmem = pl.BlockSpec(memory_space=pltpu.VMEM)
    dma = pltpu.SemaphoreType.DMA
    width = tokens.shape[1]
    ring_sems = [dma((2, NZ // 2, 2)), dma((NZ, NC, 2)), dma((NZ, 2))]
    return pl.pallas_call(
        attention_kernel,
        out_shape=jax.ShapeDtypeStruct((TOKS, HEAD), jnp.bfloat16),
        in_specs=[vmem, vmem, vmem, vmem, pl.BlockSpec(memory_space=pltpu.SMEM), vmem],
        out_specs=vmem,
        scratch_shapes=[
            pltpu.VMEM((NY, ROWS, width), jnp.bfloat16),
            pltpu.VMEM((NZ, NY, NC, wq.shape[0], 3 * HEAD), jnp.bfloat16),
            pltpu.VMEM((NZ, NC, TOKS, HEAD), jnp.bfloat16),
            pltpu.VMEM((NZ, NC, HEAD, TOKS), jnp.bfloat16),
            pltpu.VMEM((TOKS, HEAD), jnp.bfloat16),
            pltpu.VMEM((TOKS, HEAD), jnp.bfloat16),
            pltpu.VMEM((HEAD, COLS), jnp.bfloat16),
            pltpu.VMEM((HEAD + 16, COLS), jnp.float32),
            pltpu.VMEM((8, COLS), jnp.float32),
            dma((6,)),
            dma((NY, 2)),
            dma((NY - 1, 3)),
            dma((NY, 3)),
            *ring_sems,
            *ring_sems,
        ],
        compiler_params=pltpu.CompilerParams(
            collective_id=0, has_side_effects=True, vmem_limit_bytes=56 * 1024 * 1024
        ),
        name="attention",
    )(tokens, wq, wk, wv, lam, gain.reshape(-1, 1))


def on_device(tokens, query_weight, key_weight, value_weight, out_weight, mix_lambda, head_gain):
    head_out = attention(tokens, query_weight, key_weight, value_weight, mix_lambda, head_gain)
    mine = lax.all_to_all(head_out.reshape(NY, ROWS, HEAD), "y", 0, 0)
    mine = jnp.transpose(mine, (1, 0, 2)).reshape(ROWS, NY * HEAD)
    out_t = lax.all_gather(out_weight.T, ("z", "y", "core"), axis=0, tiled=True)
    partial_out = lax.dot_general(mine, out_t, (((1,), (1,)), ((), ())), preferred_element_type=jnp.float32)
    own = lax.psum_scatter(partial_out.astype(jnp.bfloat16), "x", scatter_dimension=0, tiled=True)
    return lax.all_gather(own, "x", axis=0, tiled=True)


def solution(mesh):
    fine = Mesh(mesh.devices.reshape(NZ, NY, NC, NX), ("z", "y", "core", "x"))
    sp = ("z", "y", "core")
    placed = (P(sp, None), P(sp, "x"), P(sp, "x"), P(sp, "x"), P("x", sp), P("x"), P())
    return jax.shard_map(on_device, mesh=fine, in_specs=placed, out_specs=P(sp, None), check_vma=False)
```

```python
import functools
import math

import jax
import jax.numpy as jnp
from jax import lax
from jax.experimental import pallas as pl
from jax.experimental.pallas import tpu as pltpu
from jax.sharding import Mesh
from jax.sharding import PartitionSpec as P

MESH = pl.DeviceIdType.MESH
NZ, NY, NC, NX = 8, 4, 2, 4
ROWS = 160
TOKS = NY * ROWS
HEAD = 128
COLS = 2 * TOKS
TILE = 256
LOW = -1e30
EXP_SCALE = 64 ** (-0.5) * math.log2(math.e)


def rcopy(src, dst, send_sem, recv_sem, device):
    return pltpu.make_async_remote_copy(
        src_ref=src, dst_ref=dst, send_sem=send_sem, recv_sem=recv_sem, device_id=device, device_id_type=MESH
    )


class ZRing:
    def __init__(self, block, send, recv, sib_send):
        self.block, self.send, self.recv, self.sib_send = block, send, recv, sib_send
        self.z, self.c = lax.axis_index("z"), lax.axis_index("core")

    def origin(self, way, d):
        return lax.rem(self.z + (NZ - d if way == 0 else d), NZ)

    def farthest(self, way, kind):
        return NZ // 2 - (way != kind)

    def onward(self, way, d, kind, o):
        ref = self.block(o, self.c, kind)
        to = lax.rem(self.z + (1 if way == 0 else NZ - 1), NZ)
        return rcopy(ref, ref, self.send.at[way, d - 1, kind], self.recv.at[o, self.c, kind], {"z": to})

    def share(self, o, kind):
        ref = self.block(o, self.c, kind)
        return rcopy(ref, ref, self.sib_send.at[o, kind], self.recv.at[o, self.c, kind], {"core": 1 - self.c})

    def arrived(self, o, c, kind):
        ref = self.block(o, c, kind)
        rcopy(ref, ref, self.sib_send.at[o, kind], self.recv.at[o, c, kind], {"core": 1 - self.c}).wait_recv()

    def begin(self, kind):
        for way in (0, 1):
            self.onward(way, 1, kind, self.z).start()
        self.share(self.z, kind).start()

    def pass_on(self, way, d, kind):
        o = self.origin(way, d)
        self.arrived(o, self.c, kind)

        @pl.when(d < self.farthest(way, kind))
        def _():
            self.onward(way, d + 1, kind, o).start()

        self.share(o, kind).start()

    def drain(self):
        for kind in (0, 1):
            for way in (0, 1):
                for d in range(1, self.farthest(way, kind) + 1):
                    self.onward(way, d, kind, self.z).wait_send()

            @pl.loop(0, NZ)
            def _(o):
                self.share(o, kind).wait_send()


def attention_kernel(
    tok, wq, wk, wv, wo, lam, gain, out,
    xbuf, wbuf, kbuf, vbuf, qrow, vrow, qbd, acc, top, wt, hrow, hbuf,
    tok_s, tok_r, wy_s, wy_r, w_s, w_r, w_sib, kv_s, kv_r, kv_sib,
    oz_s, oz_r, oy_s, oy_r, ox_s, of_s, ox_r, oc_s, oc_r, h_s, hf_s, h_r, hf_r,
):
    z, y, c, x = (lax.axis_index(name) for name in ("z", "y", "core", "x"))
    right, left, facing = lax.rem(x + 1, NX), lax.rem(x + NX - 1, NX), lax.rem(x + 2, NX)
    above, below = lax.rem(y + 1, NY), lax.rem(y + NY - 1, NY)
    across = lax.rem(y + 2, NY)

    barrier = pltpu.get_barrier_semaphore()
    friends = [{"y": lax.rem(y + k, NY)} for k in range(1, NY)]
    friends += [{"z": lax.rem(z + k, NZ)} for k in range(1, NZ)]
    friends += [{"y": lax.rem(y + k, NY), "x": to} for k in range(NY) for to in (left, right)]
    friends += [{"core": 1 - c}]
    for friend in friends:
        pl.semaphore_signal(barrier, inc=1, device_id=friend, device_id_type=MESH)
    pl.semaphore_wait(barrier, len(friends))

    half = ROWS // 2

    def part(slot, k):
        return xbuf.at[slot, pl.ds(k * half, half), :]

    def tok_copy(src, slot, k, n, to):
        return rcopy(src, part(slot, k), tok_s.at[n], tok_r.at[slot, k], {"y": to})

    def tok_arrived(slot, k):
        tok_copy(part(slot, k), slot, k, 0, above).wait_recv()

    def w_copy(to, k, n):
        src = (wq, wk, wv)[n].at[:, pl.ds(pl.multiple_of(to * HEAD, HEAD), HEAD)]
        dst = wbuf.at[z, y, c, :, pl.ds(n * HEAD, HEAD)]
        return rcopy(src, dst, wy_s.at[k, n], wy_r.at[y, n], {"y": to})

    for k in range(1, NY):
        for n in range(3):
            w_copy(lax.rem(y + k, NY), k - 1, n).start()
    own = [
        tok_copy(tok.at[pl.ds(0, half), :], y, 0, 0, above),
        tok_copy(tok.at[pl.ds(half, half), :], y, 1, 1, below),
        tok_copy(tok.at[pl.ds(half, half), :], y, 1, 2, above),
        tok_copy(tok.at[pl.ds(0, half), :], y, 0, 3, below),
    ]
    for copy in own:
        copy.start()

    def piece(xx, yy):
        return wt.at[xx, :, yy, c]

    def half_piece(xx, yy, k):
        return wt.at[xx, pl.ds(k * (NZ // 2), NZ // 2), yy, c]

    def turn(i):
        return lax.rem(y + jnp.where(i == 2, 3, jnp.where(i == 3, 2, i)), NY)

    def o_z(k):
        block = wt.at[x, z, y, c]
        return rcopy(block, block, oz_s.at[k - 1], oz_r.at[z], {"z": lax.rem(z + k, NZ)})

    def o_z_arrived(k):
        frm = lax.rem(z + k, NZ)
        block = wt.at[x, frm, y, c]
        rcopy(block, block, oz_s.at[k - 1], oz_r.at[frm], {"z": frm}).wait_recv()

    def o_y(k):
        return rcopy(piece(x, y), piece(x, y), oy_s.at[k - 1], oy_r.at[y], {"y": lax.rem(y + k, NY)})

    def o_y_arrived(yy):
        rcopy(piece(x, yy), piece(x, yy), oy_s.at[0], oy_r.at[yy], {"y": above}).wait_recv()

    def o_x(yy):
        return [
            rcopy(half_piece(x, yy, k), half_piece(x, yy, k), ox_s.at[yy, n], ox_r.at[x, yy, k], {"x": to})
            for n, (k, to) in enumerate([(0, right), (1, left), (1, right), (0, left)])
        ]

    def o_x_arrived(xx, yy, k):
        ref = half_piece(xx, yy, k)
        rcopy(ref, ref, ox_s.at[yy, 0], ox_r.at[xx, yy, k], {"x": right}).wait_recv()

    def o_relay(yy, k):
        frm, to = ((left, right), (right, left))[k]
        ref = half_piece(frm, yy, k)
        return rcopy(ref, ref, of_s.at[yy, k], ox_r.at[frm, yy, k], {"x": to})

    def o_share(xx, yy):
        return rcopy(piece(xx, yy), piece(xx, yy), oc_s.at[xx, yy], oc_r.at[xx, yy], {"core": 1 - c})

    def o_shared(xx, yy):
        ref = wt.at[xx, :, yy, 1 - c]
        rcopy(ref, ref, oc_s.at[xx, yy], oc_r.at[xx, yy], {"core": 1 - c}).wait_recv()

    def o_spread(yy):
        for copy in o_x(yy):
            copy.start()
        o_share(x, yy).start()

    wt[x, z, y, c] = wo[...].T
    for k in range(1, NZ):
        o_z(k).start()

    mine = pl.ds(pl.multiple_of(y * HEAD, HEAD), HEAD)
    for n, w in enumerate((wq, wk, wv)):
        wbuf[z, y, c, :, n * HEAD : (n + 1) * HEAD] = w[:, mine]
    xbuf[y] = tok[...]
    acc[...] = jnp.zeros_like(acc)
    top[...] = jnp.full_like(top, LOW)

    for k in range(1, NY):
        frm = lax.rem(y + k, NY)
        for n in range(3):
            dst = wbuf.at[z, frm, c, :, pl.ds(n * HEAD, HEAD)]
            rcopy(dst, dst, wy_s.at[k - 1, n], wy_r.at[frm, n], {"y": frm}).wait_recv()

    wring = ZRing(lambda o, cc, kind: wbuf.at[o, pl.ds(2 * kind, 2), cc], w_s, w_r, w_sib)
    for kind in (0, 1):
        wring.begin(kind)
    fwd_up = tok_copy(part(below, 0), below, 0, 4, above)
    fwd_down = tok_copy(part(above, 1), above, 1, 5, below)
    for d in range(1, NZ // 2 + 1):
        for kind in (0, 1):
            for way in (0, 1):
                if d <= wring.farthest(way, kind):
                    wring.pass_on(way, d, kind)
        if d == 2:
            tok_arrived(below, 0)
            fwd_up.start()
            tok_arrived(above, 1)
            fwd_down.start()
    for o in range(NZ):
        for kind in (0, 1):
            wring.arrived(o, 1 - c, kind)

    for k in range(1, NZ):
        o_z_arrived(k)
    for k in range(1, NY):
        o_y(k).start()
    o_spread(y)

    def project(i, carry):
        slot = turn(i)

        @pl.when(i == 1)
        def _():
            tok_arrived(above, 0)

        @pl.when(i == 2)
        def _():
            tok_arrived(below, 1)

        @pl.when(i == 3)
        def _():
            tok_arrived(across, 0)
            tok_arrived(across, 1)

        made = jnp.dot(
            xbuf[slot], wbuf[...].reshape(-1, 3 * HEAD), preferred_element_type=jnp.float32
        ).astype(jnp.bfloat16)
        at = pl.ds(pl.multiple_of(slot * ROWS, ROWS), ROWS)
        qrow[at, :] = made[:, :HEAD]
        kbuf[z, c, at, :] = made[:, HEAD : 2 * HEAD]
        vrow[at, :] = made[:, 2 * HEAD :]
        return carry

    lax.fori_loop(0, NY, project, 0)
    vbuf[z, c] = vrow[...].T

    ring = ZRing(lambda o, cc, kind: (kbuf, vbuf)[kind].at[o, cc], kv_s, kv_r, kv_sib)
    for kind in (0, 1):
        ring.begin(kind)

    q_t = qrow[...].T
    first = lax.broadcasted_iota(jnp.int32, q_t.shape, 0) < HEAD // 2
    zero = jnp.zeros_like(q_t)
    qbd[:, :TOKS] = jnp.where(first, q_t, zero)
    qbd[:, TOKS:] = jnp.where(first, zero, q_t)

    ones = jnp.ones((16, TOKS), jnp.bfloat16)

    def visit(o, cc, masked):
        keys = kbuf[o, cc]
        values = jnp.concatenate([vbuf[o, cc], ones], axis=0)
        for j in range(COLS // TILE):
            cols = slice(j * TILE, (j + 1) * TILE)
            s = jnp.dot(keys, qbd[:, cols], preferred_element_type=jnp.float32)
            if masked:
                u = lax.broadcasted_iota(jnp.int32, (TOKS, 1), 0)
                t = lax.broadcasted_iota(jnp.int32, (1, TILE), 1) + j * TILE
                t = jnp.where(t >= TOKS, t - TOKS, t)

                def place(r, core):
                    skipped = sum((r >= k * ROWS).astype(jnp.int32) for k in range(1, NY))
                    return r + ROWS * (skipped + core)

                s = jnp.where(place(u, cc) <= place(t, c), s, LOW)
            before = top[0:1, cols]
            now = jnp.maximum(before, jnp.max(s, axis=0, keepdims=True))
            shrink = jnp.exp2((before - now) * EXP_SCALE)
            p = jnp.exp2((s - now) * EXP_SCALE).astype(jnp.bfloat16)
            acc[:, cols] = acc[:, cols] * shrink + jnp.dot(values, p, preferred_element_type=jnp.float32)
            top[0:1, cols] = now

    def own_slice(k, carry):
        cc = jnp.where(k == 0, c, 1 - c)

        @pl.when(k == 1)
        def _():
            for kind in (0, 1):
                ring.arrived(z, 1 - c, kind)

        visit(z, cc, True)
        return carry

    lax.fori_loop(0, NC, own_slice, 0)

    def step(d, carry):
        for kind in (0, 1):
            for way in (0, 1):
                @pl.when(d <= ring.farthest(way, kind))
                def _():
                    ring.pass_on(way, d, kind)

            way = kind
            before = d - 1
            o = ring.origin(way, before)
            there = (before >= 1) & (before <= NZ // 2 - way)

            @pl.when(there)
            def _():
                for other in (0, 1):
                    ring.arrived(o, 1 - c, other)

            @pl.when(there & (o < z))
            def _():
                def both(cc, carry):
                    visit(o, cc, False)
                    return carry

                lax.fori_loop(0, NC, both, 0)

        @pl.when(d < NY)
        def _():
            o_y_arrived(turn(d))
            o_spread(turn(d))

        @pl.when(d >= 2)
        def _():
            yy = turn(d - 2)
            for k, frm in enumerate((left, right)):
                o_x_arrived(frm, yy, k)
                o_relay(yy, k).start()
            for k, frm in enumerate((left, right)):
                o_x_arrived(frm, yy, 1 - k)
                o_share(frm, yy).start()

        return carry

    lax.fori_loop(1, NZ // 2 + 2, step, 0)

    def part_of(cols):
        return acc[:HEAD, cols] / acc[HEAD : HEAD + 1, cols]

    mixture = part_of(slice(0, TOKS)) - lam[y] * part_of(slice(TOKS, COLS))
    scale = lax.rsqrt(jnp.mean(mixture * mixture, axis=0, keepdims=True) + 1e-05)
    hrow[...] = ((mixture * scale).T * gain[...]).astype(jnp.bfloat16).reshape(NY, ROWS, HEAD)

    def rows(k):
        return pl.ds(k * half, half)

    def h_copy(yy, k, n, device):
        dst = hbuf.at[x, rows(k), pl.ds(pl.multiple_of(y * HEAD, HEAD), HEAD)]
        return rcopy(hrow.at[yy, rows(k), :], dst, h_s.at[yy, n], h_r.at[x, y, k], device)

    def h_arrived(xx, yy, k):
        dst = hbuf.at[xx, rows(k), pl.ds(pl.multiple_of(yy * HEAD, HEAD), HEAD)]
        rcopy(hrow.at[yy, rows(k), :], dst, h_s.at[yy, 0], h_r.at[xx, yy, k], {"x": right}).wait_recv()

    def h_relay(k):
        frm, to = ((left, right), (right, left))[k]
        ref = hbuf.at[frm, rows(k), :]
        return rcopy(ref, ref, hf_s.at[k], hf_r.at[k], {"x": to})

    sent = []
    for n, (k, to) in enumerate([(0, right), (1, left), (1, right), (0, left)]):
        for i in range(NY):
            yy = lax.rem(y + i, NY)
            sent.append(h_copy(yy, k, n, {"y": yy, "x": to}))
            sent[-1].start()
        if n == 1:
            for i in range(1, NY):
                yy = lax.rem(y + i, NY)
                for kk in (0, 1):
                    sent.append(h_copy(yy, kk, 4 + kk, {"y": yy}))
                    sent[-1].start()
    hbuf[x, :, mine] = hrow[y]
    relays = [h_relay(0), h_relay(1)]
    for k, frm in enumerate((left, right)):
        for i in range(NY):
            h_arrived(frm, lax.rem(y + i, NY), k)
        relays[k].start()

    for i in range(NY):
        yy = turn(i)
        for k in (0, 1):
            o_x_arrived(facing, yy, k)
        o_share(facing, yy).start()
    for xx in range(NX):
        for yy in range(NY):
            o_shared(xx, yy)
    for k in (0, 1):
        for i in range(1, NY):
            h_arrived(x, lax.rem(y + i, NY), k)
    for k, frm in enumerate((left, right)):
        for i in range(NY):
            h_arrived(frm, lax.rem(y + i, NY), 1 - k)
    for k in (0, 1):
        ref = hbuf.at[facing, rows(k), :]
        rcopy(ref, ref, hf_s.at[k], hf_r.at[k], {"x": right}).wait_recv()

    width = wo.shape[0]
    for j in range(out.shape[1] // width):
        total = jnp.zeros((width, ROWS), jnp.float32)
        for xx in range(NX):
            block = wt[xx, 2 * j : 2 * j + 2].reshape(width, width)
            total += lax.dot_general(
                block, hbuf[xx], (((1,), (1,)), ((), ())), preferred_element_type=jnp.float32
            )
        out[:, j * width : (j + 1) * width] = total.T.astype(jnp.bfloat16)

    for copy in sent + relays:
        copy.wait_send()
    for k in range(1, NZ):
        o_z(k).wait_send()
    for k in range(1, NY):
        o_y(k).wait_send()
    for yy in range(NY):
        for copy in o_x(yy):
            copy.wait_send()
        for k in (0, 1):
            o_relay(yy, k).wait_send()
        for xx in range(NX):
            o_share(xx, yy).wait_send()

    for copy in own + [fwd_up, fwd_down]:
        copy.wait_send()
    for k in range(1, NY):
        for n in range(3):
            w_copy(lax.rem(y + k, NY), k - 1, n).wait_send()
    wring.drain()
    ring.drain()


def attention(tokens, wq, wk, wv, wo, lam, gain):
    vmem = pl.BlockSpec(memory_space=pltpu.VMEM)
    dma = pltpu.SemaphoreType.DMA
    width = tokens.shape[1]
    ring_sems = [dma((2, NZ // 2, 2)), dma((NZ, NC, 2)), dma((NZ, 2))]
    return pl.pallas_call(
        attention_kernel,
        out_shape=jax.ShapeDtypeStruct(tokens.shape, jnp.bfloat16),
        in_specs=[vmem, vmem, vmem, vmem, vmem, pl.BlockSpec(memory_space=pltpu.SMEM), vmem],
        out_specs=vmem,
        scratch_shapes=[
            pltpu.VMEM((NY, ROWS, width), jnp.bfloat16),
            pltpu.VMEM((NZ, NY, NC, wq.shape[0], 3 * HEAD), jnp.bfloat16),
            pltpu.VMEM((NZ, NC, TOKS, HEAD), jnp.bfloat16),
            pltpu.VMEM((NZ, NC, HEAD, TOKS), jnp.bfloat16),
            pltpu.VMEM((TOKS, HEAD), jnp.bfloat16),
            pltpu.VMEM((TOKS, HEAD), jnp.bfloat16),
            pltpu.VMEM((HEAD, COLS), jnp.bfloat16),
            pltpu.VMEM((HEAD + 16, COLS), jnp.float32),
            pltpu.VMEM((8, COLS), jnp.float32),
            pltpu.VMEM((NX, NZ, NY, NC, wo.shape[1], wo.shape[0]), jnp.bfloat16),
            pltpu.VMEM((NY, ROWS, HEAD), jnp.bfloat16),
            pltpu.VMEM((NX, ROWS, NY * HEAD), jnp.bfloat16),
            dma((6,)),
            dma((NY, 2)),
            dma((NY - 1, 3)),
            dma((NY, 3)),
            *ring_sems,
            *ring_sems,
            dma((NZ - 1,)),
            dma((NZ,)),
            dma((NY - 1,)),
            dma((NY,)),
            dma((NY, 4)),
            dma((NY, 2)),
            dma((NX, NY, 2)),
            dma((NX, NY)),
            dma((NX, NY)),
            dma((NY, 6)),
            dma((2,)),
            dma((NX, NY, 2)),
            dma((2,)),
        ],
        compiler_params=pltpu.CompilerParams(
            collective_id=0, has_side_effects=True, vmem_limit_bytes=56 * 1024 * 1024
        ),
        name="attention",
    )(tokens, wq, wk, wv, wo, lam, gain.reshape(1, -1))


def on_device(tokens, query_weight, key_weight, value_weight, out_weight, mix_lambda, head_gain):
    return attention(tokens, query_weight, key_weight, value_weight, out_weight, mix_lambda, head_gain)


def solution(mesh):
    fine = Mesh(mesh.devices.reshape(NZ, NY, NC, NX), ("z", "y", "core", "x"))
    sp = ("z", "y", "core")
    placed = (P(sp, None), P(sp, "x"), P(sp, "x"), P(sp, "x"), P("x", sp), P("x"), P())
    return jax.shard_map(on_device, mesh=fine, in_specs=placed, out_specs=P(sp, None), check_vma=False)
```

```python
import functools
import math

import jax
import jax.numpy as jnp
from jax import lax
from jax.experimental import pallas as pl
from jax.experimental.pallas import tpu as pltpu
from jax.sharding import Mesh
from jax.sharding import PartitionSpec as P

MESH = pl.DeviceIdType.MESH
NZ, NY, NC, NX = 8, 4, 2, 4
ROWS = 160
TOKS = NY * ROWS
HEAD = 128
COLS = 2 * TOKS
TILE = 256
KINDS = 4
LOW = -1e30
EXP_SCALE = 64 ** (-0.5) * math.log2(math.e)


def rcopy(src, dst, send_sem, recv_sem, device):
    return pltpu.make_async_remote_copy(
        src_ref=src, dst_ref=dst, send_sem=send_sem, recv_sem=recv_sem, device_id=device, device_id_type=MESH
    )


class ZRing:
    def __init__(self, block, send, recv, sib_send):
        self.block, self.send, self.recv, self.sib_send = block, send, recv, sib_send
        self.z, self.c = lax.axis_index("z"), lax.axis_index("core")

    def origin(self, way, d):
        return lax.rem(self.z + (NZ - d if way == 0 else d), NZ)

    def farthest(self, way, kind):
        return NZ // 2 - (way != kind % 2)

    def onward(self, way, d, kind, o):
        ref = self.block(o, self.c, kind)
        to = lax.rem(self.z + (1 if way == 0 else NZ - 1), NZ)
        return rcopy(ref, ref, self.send.at[way, d - 1, kind], self.recv.at[o, self.c, kind], {"z": to})

    def share(self, o, kind):
        ref = self.block(o, self.c, kind)
        return rcopy(ref, ref, self.sib_send.at[o, kind], self.recv.at[o, self.c, kind], {"core": 1 - self.c})

    def arrived(self, o, c, kind):
        ref = self.block(o, c, kind)
        rcopy(ref, ref, self.sib_send.at[o, kind], self.recv.at[o, c, kind], {"core": 1 - self.c}).wait_recv()

    def begin(self, kind):
        for way in (0, 1):
            self.onward(way, 1, kind, self.z).start()
        self.share(self.z, kind).start()

    def pass_on(self, way, d, kind):
        o = self.origin(way, d)
        self.arrived(o, self.c, kind)

        @pl.when(d < self.farthest(way, kind))
        def _():
            self.onward(way, d + 1, kind, o).start()

        self.share(o, kind).start()

    def drain(self):
        for kind in range(KINDS):
            for way in (0, 1):
                for d in range(1, self.farthest(way, kind) + 1):
                    self.onward(way, d, kind, self.z).wait_send()

            @pl.loop(0, NZ)
            def _(o):
                self.share(o, kind).wait_send()


def attention_kernel(
    tok, wq, wk, wv, wo, lam, gain, out,
    xbuf, wkv, wqs, kv, qrow, qbd, acc, top, wt, hrow, hbuf, osum,
    tok_s, tok_r, wy_s, wy_r, w_s, w_r, w_sib, kv_s, kv_r, kv_sib,
    oz_s, oz_r, oy_s, oy_r, ox_s, of_s, ox_r, oc_s, oc_r, h_s, hf_s, h_r, hf_r,
):
    z, y, c, x = (lax.axis_index(name) for name in ("z", "y", "core", "x"))
    right, left, facing = lax.rem(x + 1, NX), lax.rem(x + NX - 1, NX), lax.rem(x + 2, NX)
    above, below = lax.rem(y + 1, NY), lax.rem(y + NY - 1, NY)
    across = lax.rem(y + 2, NY)

    barrier = pltpu.get_barrier_semaphore()
    friends = [{"y": lax.rem(y + k, NY)} for k in range(1, NY)]
    friends += [{"z": lax.rem(z + k, NZ)} for k in range(1, NZ)]
    friends += [{"y": lax.rem(y + k, NY), "x": to} for k in range(NY) for to in (left, right)]
    friends += [{"core": 1 - c}]
    for friend in friends:
        pl.semaphore_signal(barrier, inc=1, device_id=friend, device_id_type=MESH)
    pl.semaphore_wait(barrier, len(friends))

    half = ROWS // 2

    def part(slot, k):
        return xbuf.at[slot, pl.ds(k * half, half), :]

    def tok_copy(src, slot, k, n, to):
        return rcopy(src, part(slot, k), tok_s.at[n], tok_r.at[slot, k], {"y": to})

    def tok_arrived(slot, k):
        tok_copy(part(slot, k), slot, k, 0, above).wait_recv()

    def w_slot(frm, n):
        return (wqs.at[z, frm, c], wkv.at[z, frm, c, :, pl.ds(0, HEAD)], wkv.at[z, frm, c, :, pl.ds(HEAD, HEAD)])[n]

    def w_copy(k, n):
        to = lax.rem(y + k, NY)
        src = (wq, wk, wv)[n].at[:, pl.ds(pl.multiple_of(to * HEAD, HEAD), HEAD)]
        return rcopy(src, w_slot(y, n), wy_s.at[k - 1, n], wy_r.at[y, n], {"y": to})

    def w_arrived(n):
        for k in range(1, NY):
            frm = lax.rem(y + k, NY)
            rcopy(w_slot(frm, n), w_slot(frm, n), wy_s.at[k - 1, n], wy_r.at[frm, n], {"y": frm}).wait_recv()

    for n in (1, 2, 0):
        for k in range(1, NY):
            w_copy(k, n).start()
    own = [
        tok_copy(tok.at[pl.ds(0, half), :], y, 0, 0, above),
        tok_copy(tok.at[pl.ds(half, half), :], y, 1, 1, below),
        tok_copy(tok.at[pl.ds(half, half), :], y, 1, 2, above),
        tok_copy(tok.at[pl.ds(0, half), :], y, 0, 3, below),
    ]
    for copy in own:
        copy.start()

    def piece(xx, yy):
        return wt.at[xx, :, yy, c]

    def half_piece(xx, yy, k):
        return wt.at[xx, pl.ds(k * (NZ // 2), NZ // 2), yy, c]

    def turn(i):
        return lax.rem(y + jnp.where(i == 2, 3, jnp.where(i == 3, 2, i)), NY)

    def o_z(k):
        block = wt.at[x, z, y, c]
        return rcopy(block, block, oz_s.at[k - 1], oz_r.at[z], {"z": lax.rem(z + k, NZ)})

    def o_z_arrived(k):
        frm = lax.rem(z + k, NZ)
        block = wt.at[x, frm, y, c]
        rcopy(block, block, oz_s.at[k - 1], oz_r.at[frm], {"z": frm}).wait_recv()

    def o_y(k):
        return rcopy(piece(x, y), piece(x, y), oy_s.at[k - 1], oy_r.at[y], {"y": lax.rem(y + k, NY)})

    def o_y_arrived(yy):
        rcopy(piece(x, yy), piece(x, yy), oy_s.at[0], oy_r.at[yy], {"y": above}).wait_recv()

    def o_x(yy):
        return [
            rcopy(half_piece(x, yy, k), half_piece(x, yy, k), ox_s.at[yy, n], ox_r.at[x, yy, k], {"x": to})
            for n, (k, to) in enumerate([(0, right), (1, left), (1, right), (0, left)])
        ]

    def o_x_arrived(xx, yy, k):
        ref = half_piece(xx, yy, k)
        rcopy(ref, ref, ox_s.at[yy, 0], ox_r.at[xx, yy, k], {"x": right}).wait_recv()

    def o_relay(yy, k):
        frm, to = ((left, right), (right, left))[k]
        ref = half_piece(frm, yy, k)
        return rcopy(ref, ref, of_s.at[yy, k], ox_r.at[frm, yy, k], {"x": to})

    def o_share(xx, yy):
        return rcopy(piece(xx, yy), piece(xx, yy), oc_s.at[xx, yy], oc_r.at[xx, yy], {"core": 1 - c})

    def o_shared(xx, yy):
        ref = wt.at[xx, :, yy, 1 - c]
        rcopy(ref, ref, oc_s.at[xx, yy], oc_r.at[xx, yy], {"core": 1 - c}).wait_recv()

    def o_spread(yy):
        for copy in o_x(yy):
            copy.start()
        o_share(x, yy).start()

    wt[x, z, y, c] = wo[...]

    mine = pl.ds(pl.multiple_of(y * HEAD, HEAD), HEAD)
    wqs[z, y, c] = wq[:, mine]
    wkv[z, y, c, :, :HEAD] = wk[:, mine]
    wkv[z, y, c, :, HEAD:] = wv[:, mine]
    xbuf[y] = tok[...]
    acc[...] = jnp.zeros_like(acc)
    top[...] = jnp.full_like(top, LOW)

    w_ring = ZRing(lambda o, cc, kind: (wkv, wqs)[kind // 2].at[o, pl.ds(2 * (kind % 2), 2), cc], w_s, w_r, w_sib)
    ring = ZRing(lambda o, cc, kind: kv.at[o, cc, pl.ds(kind * ROWS, ROWS), :], kv_s, kv_r, kv_sib)

    def pass_all(what, d, kinds):
        for kind in kinds:
            for way in (0, 1):
                if d <= what.farthest(way, kind):
                    what.pass_on(way, d, kind)

    w_arrived(1)
    w_arrived(2)
    for kind in (0, 1):
        w_ring.begin(kind)
    w_arrived(0)
    for kind in (2, 3):
        w_ring.begin(kind)
    fwd_up = tok_copy(part(below, 0), below, 0, 4, above)
    fwd_down = tok_copy(part(above, 1), above, 1, 5, below)
    for d in range(1, NZ // 2 + 1):
        pass_all(w_ring, d, (0, 1))
        if d > 1:
            pass_all(w_ring, d - 1, (2, 3))
        for k in {d, NZ - d}:
            o_z(k).start()
        if d == 2:
            tok_arrived(below, 0)
            fwd_up.start()
            tok_arrived(above, 1)
            fwd_down.start()
    for o in range(NZ):
        for kind in (0, 1):
            w_ring.arrived(o, 1 - c, kind)

    def project(i):
        at = pl.ds(pl.multiple_of(i * ROWS, ROWS), ROWS)
        kv[z, c, at, :] = jnp.dot(
            xbuf[turn(i)], wkv[...].reshape(-1, 2 * HEAD), preferred_element_type=jnp.float32
        ).astype(jnp.bfloat16)
        ring.begin(i)

    def project_near(i, carry):
        @pl.when(i == 1)
        def _():
            tok_arrived(above, 0)

        @pl.when(i == 2)
        def _():
            tok_arrived(below, 1)

        project(i)
        return carry

    lax.fori_loop(0, NY - 1, project_near, 0)

    pass_all(w_ring, NZ // 2, (2, 3))
    for k in range(1, NZ):
        o_z_arrived(k)
    for k in range(1, NY):
        o_y(k).start()
    o_spread(y)
    pass_all(ring, 1, range(NY - 1))
    for o in range(NZ):
        for kind in (2, 3):
            w_ring.arrived(o, 1 - c, kind)
    for k in (0, 1):
        tok_arrived(across, k)
    project(NY - 1)

    def queries(i, carry):
        at = pl.ds(pl.multiple_of(i * ROWS, ROWS), ROWS)
        qrow[at, :] = jnp.dot(
            xbuf[turn(i)], wqs[...].reshape(-1, HEAD), preferred_element_type=jnp.float32
        ).astype(jnp.bfloat16)
        return carry

    lax.fori_loop(0, NY, queries, 0)
    q_t = qrow[...].T
    first = lax.broadcasted_iota(jnp.int32, q_t.shape, 0) < HEAD // 2
    zero = jnp.zeros_like(q_t)
    qbd[:, :TOKS] = jnp.where(first, q_t, zero)
    qbd[:, TOKS:] = jnp.where(first, zero, q_t)

    ones = jnp.ones((16, TOKS), jnp.bfloat16)

    def place(r, core):
        i = sum((r >= k * ROWS).astype(jnp.int32) for k in range(1, NY))
        return r + ROWS * (2 * turn(i) - i + core)

    def visit(o, cc, masked):
        keys = kv[o, cc, :, :HEAD]
        values = jnp.concatenate([kv[o, cc, :, HEAD:].T, ones], axis=0)

        def scores(j):
            return jnp.dot(keys, qbd[:, j * TILE : (j + 1) * TILE], preferred_element_type=jnp.float32)

        ahead = scores(0)
        for j in range(COLS // TILE):
            cols = slice(j * TILE, (j + 1) * TILE)
            s = ahead
            if j + 1 < COLS // TILE:
                ahead = scores(j + 1)
            if masked:
                u = lax.broadcasted_iota(jnp.int32, (TOKS, 1), 0)
                t = lax.broadcasted_iota(jnp.int32, (1, TILE), 1) + j * TILE
                t = jnp.where(t >= TOKS, t - TOKS, t)
                s = jnp.where(place(u, cc) <= place(t, c), s, LOW)
            before = top[0:1, cols]
            now = jnp.maximum(before, jnp.max(s, axis=0, keepdims=True))
            shrink = jnp.exp2((before - now) * EXP_SCALE)
            p = jnp.exp2((s - now) * EXP_SCALE).astype(jnp.bfloat16)
            acc[:, cols] = acc[:, cols] * shrink + jnp.dot(values, p, preferred_element_type=jnp.float32)
            top[0:1, cols] = now

    def own_slice(k, carry):
        cc = jnp.where(k == 0, c, 1 - c)

        @pl.when(k == 1)
        def _():
            for kind in range(KINDS):
                ring.arrived(z, 1 - c, kind)

        visit(z, cc, True)
        return carry

    lax.fori_loop(0, NC, own_slice, 0)

    def step(d, carry):
        for way in (0, 1):
            for kind in (2 * way, 2 * way + 1):
                for course in (0, 1):
                    due = d <= ring.farthest(course, kind)

                    @pl.when(due if kind == KINDS - 1 else due & (d > 1))
                    def _():
                        ring.pass_on(course, d, kind)

            before = d - 1
            o = ring.origin(way, before)
            there = (before >= 1) & (before <= NZ // 2 - way)

            @pl.when(there)
            def _():
                for other in range(KINDS):
                    ring.arrived(o, 1 - c, other)

            @pl.when(there & (o < z))
            def _():
                def both(cc, carry):
                    visit(o, cc, False)
                    return carry

                lax.fori_loop(0, NC, both, 0)

        @pl.when(d < NY)
        def _():
            o_y_arrived(turn(d))
            o_spread(turn(d))

        @pl.when(d >= 2)
        def _():
            yy = turn(d - 2)
            for k, frm in enumerate((left, right)):
                o_x_arrived(frm, yy, k)
                o_relay(yy, k).start()
            for k, frm in enumerate((left, right)):
                o_x_arrived(frm, yy, 1 - k)
                o_share(frm, yy).start()

        return carry

    lax.fori_loop(1, NZ // 2 + 2, step, 0)

    def part_of(cols):
        return acc[:HEAD, cols] / acc[HEAD : HEAD + 1, cols]

    mixture = part_of(slice(0, TOKS)) - lam[y] * part_of(slice(TOKS, COLS))
    scale = lax.rsqrt(jnp.mean(mixture * mixture, axis=0, keepdims=True) + 1e-05)
    hrow[...] = ((mixture * scale).T * gain[...]).astype(jnp.bfloat16).reshape(NY, ROWS, HEAD)

    def rows(k):
        return pl.ds(k * half, half)

    def h_copy(i, k, n, device):
        dst = hbuf.at[x, rows(k), pl.ds(pl.multiple_of(y * HEAD, HEAD), HEAD)]
        return rcopy(hrow.at[i, rows(k), :], dst, h_s.at[i, n], h_r.at[x, y, k], {"y": turn(i), **device})

    def h_arrived(xx, yy, k):
        dst = hbuf.at[xx, rows(k), pl.ds(pl.multiple_of(yy * HEAD, HEAD), HEAD)]
        rcopy(hrow.at[0, rows(k), :], dst, h_s.at[0, 0], h_r.at[xx, yy, k], {"x": right}).wait_recv()

    def h_relay(k):
        frm, to = ((left, right), (right, left))[k]
        ref = hbuf.at[frm, rows(k), :]
        return rcopy(ref, ref, hf_s.at[k], hf_r.at[k], {"x": to})

    sent = []
    for n, (k, to) in enumerate([(0, right), (1, left), (1, right), (0, left)]):
        for i in range(NY):
            sent.append(h_copy(i, k, n, {"x": to}))
            sent[-1].start()
        if n == 1:
            for i in range(1, NY):
                for kk in (0, 1):
                    sent.append(h_copy(i, kk, 4 + kk, {}))
                    sent[-1].start()
    hbuf[x, :, mine] = hrow[0]
    relays = [h_relay(0), h_relay(1)]
    for k, frm in enumerate((left, right)):
        for i in range(NY):
            h_arrived(frm, lax.rem(y + i, NY), k)
        relays[k].start()

    for i in range(NY):
        yy = turn(i)
        for k in (0, 1):
            o_x_arrived(facing, yy, k)
        o_share(facing, yy).start()
    for xx in (x, left, right):
        for yy in range(NY):
            o_shared(xx, yy)
    for k in (0, 1):
        for i in range(1, NY):
            h_arrived(x, lax.rem(y + i, NY), k)
    for k, frm in enumerate((left, right)):
        for i in range(NY):
            h_arrived(frm, lax.rem(y + i, NY), 1 - k)

    width = wo.shape[1]

    def product(j, xx):
        block = wt[xx, 2 * j : 2 * j + 2].reshape(width, width)
        return lax.dot_general(block, hbuf[xx], (((1,), (1,)), ((), ())), preferred_element_type=jnp.float32)

    for j in range(out.shape[1] // width):
        osum[j] = product(j, x) + product(j, left) + product(j, right)
    for yy in range(NY):
        o_shared(facing, yy)
    for k in (0, 1):
        ref = hbuf.at[facing, rows(k), :]
        rcopy(ref, ref, hf_s.at[k], hf_r.at[k], {"x": right}).wait_recv()
    for j in range(out.shape[1] // width):
        out[:, j * width : (j + 1) * width] = (osum[j] + product(j, facing)).T.astype(jnp.bfloat16)

    for copy in sent + relays:
        copy.wait_send()
    for k in range(1, NZ):
        o_z(k).wait_send()
    for k in range(1, NY):
        o_y(k).wait_send()
    for yy in range(NY):
        for copy in o_x(yy):
            copy.wait_send()
        for k in (0, 1):
            o_relay(yy, k).wait_send()
        for xx in range(NX):
            o_share(xx, yy).wait_send()

    for copy in own + [fwd_up, fwd_down]:
        copy.wait_send()
    for k in range(1, NY):
        for n in range(3):
            w_copy(k, n).wait_send()
    w_ring.drain()
    ring.drain()


def attention(tokens, wq, wk, wv, wo, lam, gain):
    vmem = pl.BlockSpec(memory_space=pltpu.VMEM)
    dma = pltpu.SemaphoreType.DMA
    width = tokens.shape[1]
    ring_sems = [dma((2, NZ // 2, KINDS)), dma((NZ, NC, KINDS)), dma((NZ, KINDS))]
    return pl.pallas_call(
        attention_kernel,
        out_shape=jax.ShapeDtypeStruct(tokens.shape, jnp.bfloat16),
        in_specs=[vmem, vmem, vmem, vmem, vmem, pl.BlockSpec(memory_space=pltpu.SMEM), vmem],
        out_specs=vmem,
        scratch_shapes=[
            pltpu.VMEM((NY, ROWS, width), jnp.bfloat16),
            pltpu.VMEM((NZ, NY, NC, wq.shape[0], 2 * HEAD), jnp.bfloat16),
            pltpu.VMEM((NZ, NY, NC, wq.shape[0], HEAD), jnp.bfloat16),
            pltpu.VMEM((NZ, NC, TOKS, 2 * HEAD), jnp.bfloat16),
            pltpu.VMEM((TOKS, HEAD), jnp.bfloat16),
            pltpu.VMEM((HEAD, COLS), jnp.bfloat16),
            pltpu.VMEM((HEAD + 16, COLS), jnp.float32),
            pltpu.VMEM((8, COLS), jnp.float32),
            pltpu.VMEM((NX, NZ, NY, NC, wo.shape[0], wo.shape[1]), jnp.bfloat16),
            pltpu.VMEM((NY, ROWS, HEAD), jnp.bfloat16),
            pltpu.VMEM((NX, ROWS, NY * HEAD), jnp.bfloat16),
            pltpu.VMEM((width // wo.shape[1], wo.shape[1], ROWS), jnp.float32),
            dma((6,)),
            dma((NY, 2)),
            dma((NY - 1, 3)),
            dma((NY, 3)),
            *ring_sems,
            *ring_sems,
            dma((NZ - 1,)),
            dma((NZ,)),
            dma((NY - 1,)),
            dma((NY,)),
            dma((NY, 4)),
            dma((NY, 2)),
            dma((NX, NY, 2)),
            dma((NX, NY)),
            dma((NX, NY)),
            dma((NY, 6)),
            dma((2,)),
            dma((NX, NY, 2)),
            dma((2,)),
        ],
        compiler_params=pltpu.CompilerParams(
            collective_id=0, has_side_effects=True, vmem_limit_bytes=56 * 1024 * 1024
        ),
        name="attention",
    )(tokens, wq, wk, wv, wo, lam, gain.reshape(1, -1))


def on_device(tokens, query_weight, key_weight, value_weight, out_weight, mix_lambda, head_gain):
    return attention(tokens, query_weight, key_weight, value_weight, out_weight.T, mix_lambda, head_gain)


def solution(mesh):
    fine = Mesh(mesh.devices.reshape(NZ, NY, NC, NX), ("z", "y", "core", "x"))
    sp = ("z", "y", "core")
    placed = (P(sp, None), P(sp, "x"), P(sp, "x"), P(sp, "x"), P("x", sp), P("x"), P())
    return jax.shard_map(on_device, mesh=fine, in_specs=placed, out_specs=P(sp, None), check_vma=False)
```

```python
import functools
import math

import jax
import jax.numpy as jnp
from jax import lax
from jax.experimental import pallas as pl
from jax.experimental.pallas import tpu as pltpu
from jax.sharding import Mesh
from jax.sharding import PartitionSpec as P

MESH = pl.DeviceIdType.MESH
NZ, NY, NC, NX = 8, 4, 2, 4
ROWS = 160
TOKS = NY * ROWS
HEAD = 128
COLS = 2 * TOKS
TILE = 256
KINDS = 4
W_KINDS = 8
LOW = -1e30
EXP_SCALE = 64 ** (-0.5) * math.log2(math.e)


def rcopy(src, dst, send_sem, recv_sem, device):
    return pltpu.make_async_remote_copy(
        src_ref=src, dst_ref=dst, send_sem=send_sem, recv_sem=recv_sem, device_id=device, device_id_type=MESH
    )


class ZRing:
    def __init__(self, kinds, shared, pairs, block, send, recv, sib_send):
        self.pairs = pairs
        self.kinds, self.shared = kinds, shared
        self.block, self.send, self.recv, self.sib_send = block, send, recv, sib_send
        self.z, self.c = lax.axis_index("z"), lax.axis_index("core")

    def origin(self, way, d):
        return lax.rem(self.z + (NZ - d if way == 0 else d), NZ)

    def farthest(self, way, kind):
        return NZ // 2 - (way != kind % 2)

    def onward(self, way, d, kind, o):
        ref = self.block(o, self.c, kind)
        reach = 2 - d % 2 if self.pairs else 1
        to = lax.rem(self.z + (reach if way == 0 else NZ - reach), NZ)
        return rcopy(ref, ref, self.send.at[way, d - 1, kind], self.recv.at[o, self.c, kind], {"z": to})

    def share(self, o, kind):
        ref = self.block(o, self.c, kind)
        return rcopy(ref, ref, self.sib_send.at[o, kind], self.recv.at[o, self.c, kind], {"core": 1 - self.c})

    def arrived(self, o, c, kind):
        ref = self.block(o, c, kind)
        rcopy(ref, ref, self.sib_send.at[o, kind], self.recv.at[o, c, kind], {"core": 1 - self.c}).wait_recv()

    def shares(self, kind):
        return self.shared == self.kinds or kind < self.shared

    def begin(self, kinds):
        for d in (2, 1) if self.pairs else (1,):
            for kind in kinds:
                for way in (0, 1):
                    self.onward(way, d, kind, self.z).start()
        for kind in kinds:
            if self.shares(kind):
                self.share(self.z, kind).start()

    def pass_on(self, way, d, kind):
        o = self.origin(way, d)
        self.arrived(o, self.c, kind)

        if self.pairs:
            for far in range(3, self.farthest(way, kind) + 1) if d == 2 else ():
                self.onward(way, far, kind, o).start()
        else:

            @pl.when(d < self.farthest(way, kind))
            def _():
                self.onward(way, d + 1, kind, o).start()

        if self.shares(kind):
            self.share(o, kind).start()

    def drain(self):
        for kind in range(self.kinds):
            for way in (0, 1):
                for d in range(1, self.farthest(way, kind) + 1):
                    self.onward(way, d, kind, self.z).wait_send()

            if self.shares(kind):
                @pl.loop(0, NZ)
                def _(o):
                    self.share(o, kind).wait_send()


def attention_kernel(
    tok, wq, wk, wv, wo, lam, gain, out,
    xbuf, wkv, wqs, kv, qrow, qbd, acc, top, wt, hrow, hbuf, osum,
    tok_s, tok_r, wy_s, wy_r, w_s, w_r, w_sib, kv_s, kv_r, kv_sib,
    o2_s, o2_r, o3_s, of_s, o3_r, oc_s, oc_r, h_s, hf_s, h_r, hf_r,
):
    z, y, c, x = (lax.axis_index(name) for name in ("z", "y", "core", "x"))
    right, left, facing = lax.rem(x + 1, NX), lax.rem(x + NX - 1, NX), lax.rem(x + 2, NX)
    above, below = lax.rem(y + 1, NY), lax.rem(y + NY - 1, NY)
    across = lax.rem(y + 2, NY)

    barrier = pltpu.get_barrier_semaphore()
    friends = [{"y": lax.rem(y + k, NY)} for k in range(1, NY)]
    friends += [{"z": lax.rem(z + k, NZ)} for k in range(1, NZ)]
    friends += [{"y": lax.rem(y + k, NY), "x": to} for k in range(NY) for to in (left, right)]
    friends += [{"x": facing}, {"core": 1 - c}]
    for friend in friends:
        pl.semaphore_signal(barrier, inc=1, device_id=friend, device_id_type=MESH)
    pl.semaphore_wait(barrier, len(friends))

    half = ROWS // 2

    def part(slot, k):
        return xbuf.at[slot, pl.ds(k * half, half), :]

    def tok_copy(src, slot, k, n, to):
        return rcopy(src, part(slot, k), tok_s.at[n], tok_r.at[slot, k], {"y": to})

    def tok_arrived(slot, k):
        tok_copy(part(slot, k), slot, k, 0, above).wait_recv()

    def w_slot(frm, n):
        return (wqs.at[z, frm, c], wkv.at[z, frm, c, :, pl.ds(0, HEAD)], wkv.at[z, frm, c, :, pl.ds(HEAD, HEAD)])[n]

    def w_copy(k, n):
        to = lax.rem(y + k, NY)
        src = (wq, wk, wv)[n].at[:, pl.ds(pl.multiple_of(to * HEAD, HEAD), HEAD)]
        return rcopy(src, w_slot(y, n), wy_s.at[k - 1, n], wy_r.at[y, n], {"y": to})

    def w_arrived(n):
        for k in range(1, NY):
            frm = lax.rem(y + k, NY)
            rcopy(w_slot(frm, n), w_slot(frm, n), wy_s.at[k - 1, n], wy_r.at[frm, n], {"y": frm}).wait_recv()

    for n in (1, 2, 0):
        for k in range(1, NY):
            w_copy(k, n).start()
    own = [
        tok_copy(tok.at[pl.ds(0, half), :], y, 0, 0, above),
        tok_copy(tok.at[pl.ds(half, half), :], y, 1, 1, below),
        tok_copy(tok.at[pl.ds(half, half), :], y, 1, 2, above),
        tok_copy(tok.at[pl.ds(0, half), :], y, 0, 3, below),
    ]
    for copy in own:
        copy.start()

    places = {"y": (y, above, below), "x": (x, right, left)}

    def axes(h):
        return ("y", "x") if h == 0 else ("x", "y")

    def piece(h, a, b, core, z_half=None):
        xx, yy = (b, a) if h == 0 else (a, b)
        zs = slice(None) if z_half is None else pl.ds(z_half * (NZ // 2), NZ // 2)
        return wt.at[h, xx, zs, yy, core]

    def turn(i, at=y):
        return lax.rem(at + jnp.where(i == 2, 3, jnp.where(i == 3, 2, i)), NY)

    def o_second(h, k):
        a, b = (places[name][0] for name in axes(h))
        ref = piece(h, a, b, c)
        return rcopy(ref, ref, o2_s.at[h, k - 1], o2_r.at[h, a], {axes(h)[0]: lax.rem(a + k, NY)})

    def o_second_arrived(h, a):
        ref = piece(h, a, places[axes(h)[1]][0], c)
        rcopy(ref, ref, o2_s.at[h, 0], o2_r.at[h, a], {axes(h)[0]: places[axes(h)[0]][1]}).wait_recv()

    def o_third(h, a):
        name = axes(h)[1]
        b, up, down = places[name]
        return [
            rcopy(piece(h, a, b, c, k), piece(h, a, b, c, k), o3_s.at[h, a, n], o3_r.at[h, a, b, k], {name: to})
            for n, (k, to) in enumerate([(0, up), (1, down), (1, up), (0, down)])
        ]

    def o_third_arrived(h, a, b, k):
        ref = piece(h, a, b, c, k)
        name = axes(h)[1]
        rcopy(ref, ref, o3_s.at[h, a, 0], o3_r.at[h, a, b, k], {name: places[name][1]}).wait_recv()

    def o_relay(h, a, k):
        name = axes(h)[1]
        b, up, down = places[name]
        frm, to = ((down, up), (up, down))[k]
        ref = piece(h, a, frm, c, k)
        return rcopy(ref, ref, of_s.at[h, a, k], o3_r.at[h, a, frm, k], {name: to})

    def o_share(h, a, b):
        ref = piece(h, a, b, c)
        return rcopy(ref, ref, oc_s.at[h, a, b], oc_r.at[h, a, b], {"core": 1 - c})

    def o_shared(h, a, b):
        ref = piece(h, a, b, 1 - c)
        rcopy(ref, ref, oc_s.at[h, a, b], oc_r.at[h, a, b], {"core": 1 - c}).wait_recv()

    def o_spread(h, a):
        for copy in o_third(h, a):
            copy.start()
        o_share(h, a, places[axes(h)[1]][0]).start()

    def w_block(o, cc, kind):
        if kind < 4:
            return wkv.at[o, kind, cc]
        if kind < 6:
            return wqs.at[o, pl.ds(2 * (kind - 4), 2), cc]
        return wt.at[kind - 6, x, o, y, c]

    w_ring = ZRing(W_KINDS, 6, True, w_block, w_s, w_r, w_sib)
    ring = ZRing(KINDS, KINDS, False, lambda o, cc, kind: kv.at[o, cc, pl.ds(kind * ROWS, ROWS), :], kv_s, kv_r, kv_sib)

    def pass_all(what, d, kinds):
        for kind in kinds:
            for way in (0, 1):
                if d <= what.farthest(way, kind):
                    what.pass_on(way, d, kind)

    for h in (0, 1):
        wt[h, x, z, y, c] = wo[:, h * wo.shape[1] // 2 : (h + 1) * wo.shape[1] // 2]
    w_ring.begin((6, 7))

    mine = pl.ds(pl.multiple_of(y * HEAD, HEAD), HEAD)
    wqs[z, y, c] = wq[:, mine]
    wkv[z, y, c, :, :HEAD] = wk[:, mine]
    wkv[z, y, c, :, HEAD:] = wv[:, mine]
    xbuf[y] = tok[...]
    acc[...] = jnp.zeros_like(acc)
    top[...] = jnp.full_like(top, LOW)

    key_value, query, output = range(4), (4, 5), (6, 7)
    w_arrived(1)
    w_arrived(2)
    w_ring.begin(key_value)
    pass_all(w_ring, 2, key_value)
    pass_all(w_ring, 2, output)
    w_arrived(0)
    w_ring.begin(query)
    fwd_up = tok_copy(part(below, 0), below, 0, 4, above)
    fwd_down = tok_copy(part(above, 1), above, 1, 5, below)
    pass_all(w_ring, 1, key_value)
    tok_arrived(below, 0)
    fwd_up.start()
    tok_arrived(above, 1)
    fwd_down.start()
    pass_all(w_ring, 2, query)
    pass_all(w_ring, 3, key_value)
    pass_all(w_ring, 4, key_value)
    for o in range(NZ):
        for kind in key_value:
            w_ring.arrived(o, 1 - c, kind)

    def project(i):
        at = pl.ds(pl.multiple_of(i * ROWS, ROWS), ROWS)
        kv[z, c, at, :] = jnp.dot(
            xbuf[turn(i)], wkv[...].reshape(-1, 2 * HEAD), preferred_element_type=jnp.float32
        ).astype(jnp.bfloat16)
        ring.begin((i,))

    def project_near(i, carry):
        @pl.when(i == 1)
        def _():
            tok_arrived(above, 0)

        @pl.when(i == 2)
        def _():
            tok_arrived(below, 1)

        project(i)
        return carry

    lax.fori_loop(0, NY - 1, project_near, 0)

    for d in (1, 3, 4):
        pass_all(w_ring, d, output)
    for h in (1, 0):
        for k in (1, 3, 2):
            o_second(h, k).start()
        o_spread(h, places[axes(h)[0]][0])
    for d in (1, 3, 4):
        pass_all(w_ring, d, query)
    for n in range(3):
        for k in range(1, NY):
            w_copy(k, n).wait_send()
    w_ring.drain()
    for k in (0, 1):
        tok_arrived(across, k)
    project(NY - 1)
    pass_all(ring, 1, range(NY - 1))
    for o in range(NZ):
        for kind in query:
            w_ring.arrived(o, 1 - c, kind)

    def queries(i, carry):
        at = pl.ds(pl.multiple_of(i * ROWS, ROWS), ROWS)
        qrow[at, :] = jnp.dot(
            xbuf[turn(i)], wqs[...].reshape(-1, HEAD), preferred_element_type=jnp.float32
        ).astype(jnp.bfloat16)
        return carry

    lax.fori_loop(0, NY, queries, 0)
    q_t = qrow[...].T
    first = lax.broadcasted_iota(jnp.int32, q_t.shape, 0) < HEAD // 2
    zero = jnp.zeros_like(q_t)
    qbd[:, :TOKS] = jnp.where(first, q_t, zero)
    qbd[:, TOKS:] = jnp.where(first, zero, q_t)

    ones = jnp.ones((16, TOKS), jnp.bfloat16)

    def place(r, core):
        i = sum((r >= k * ROWS).astype(jnp.int32) for k in range(1, NY))
        return r + ROWS * (2 * turn(i) - i + core)

    def visit(o, cc, masked):
        keys = kv[o, cc, :, :HEAD]
        values = jnp.concatenate([kv[o, cc, :, HEAD:].T, ones], axis=0)

        def scores(j):
            return jnp.dot(keys, qbd[:, j * TILE : (j + 1) * TILE], preferred_element_type=jnp.float32)

        ahead = scores(0)
        for j in range(COLS // TILE):
            cols = slice(j * TILE, (j + 1) * TILE)
            s = ahead
            if j + 1 < COLS // TILE:
                ahead = scores(j + 1)
            if masked:
                u = lax.broadcasted_iota(jnp.int32, (TOKS, 1), 0)
                t = lax.broadcasted_iota(jnp.int32, (1, TILE), 1) + j * TILE
                t = jnp.where(t >= TOKS, t - TOKS, t)
                s = jnp.where(place(u, cc) <= place(t, c), s, LOW)
            before = top[0:1, cols]
            now = jnp.maximum(before, jnp.max(s, axis=0, keepdims=True))
            shrink = jnp.exp2((before - now) * EXP_SCALE)
            p = jnp.exp2((s - now) * EXP_SCALE).astype(jnp.bfloat16)
            acc[:, cols] = acc[:, cols] * shrink + jnp.dot(values, p, preferred_element_type=jnp.float32)
            top[0:1, cols] = now

    def own_slice(k, carry):
        cc = jnp.where(k == 0, c, 1 - c)

        @pl.when(k == 1)
        def _():
            for kind in range(KINDS):
                ring.arrived(z, 1 - c, kind)

        visit(z, cc, True)
        return carry

    lax.fori_loop(0, NC, own_slice, 0)

    def step(d, carry):
        for way in (0, 1):
            for kind in (2 * way, 2 * way + 1):
                for course in (0, 1):
                    due = d <= ring.farthest(course, kind)

                    @pl.when(due if kind == KINDS - 1 else due & (d > 1))
                    def _():
                        ring.pass_on(course, d, kind)

            before = d - 1
            o = ring.origin(way, before)
            there = (before >= 1) & (before <= NZ // 2 - way)

            @pl.when(there)
            def _():
                for other in range(KINDS):
                    ring.arrived(o, 1 - c, other)

            @pl.when(there & (o < z))
            def _():
                def both(cc, carry):
                    visit(o, cc, False)
                    return carry

                lax.fori_loop(0, NC, both, 0)

        @pl.when(d == 1)
        def _():
            for k in (3, 1, 2):
                for h in (1, 0):
                    came = lax.rem(places[axes(h)[0]][0] + k, NY)
                    o_second_arrived(h, came)
                    o_spread(h, came)

        def relay(i):
            for h in (1, 0):
                here, up, down = places[axes(h)[1]]
                a = lax.rem(places[axes(h)[0]][0] + (0, 3, 1, 2)[i], NY)
                for k, frm in enumerate((down, up)):
                    o_third_arrived(h, a, frm, k)
                    o_relay(h, a, k).start()
                for k, frm in enumerate((down, up)):
                    o_third_arrived(h, a, frm, 1 - k)
                    o_share(h, a, frm).start()

        def last(i):
            for h in (1, 0):
                a = lax.rem(places[axes(h)[0]][0] + (0, 3, 1, 2)[i], NY)
                b = lax.rem(places[axes(h)[1]][0] + 2, NY)
                for k in (0, 1):
                    o_third_arrived(h, a, b, k)
                o_share(h, a, b).start()

        for i, at in enumerate((1, 2, 3, 3)):

            @pl.when(d == at)
            def _():
                relay(i)

            @pl.when(d == (4 if i < 2 else 5))
            def _():
                last(i)

        return carry

    lax.fori_loop(1, NZ // 2 + 2, step, 0)

    def part_of(cols):
        return acc[:HEAD, cols] / acc[HEAD : HEAD + 1, cols]

    mixture = part_of(slice(0, TOKS)) - lam[y] * part_of(slice(TOKS, COLS))
    scale = lax.rsqrt(jnp.mean(mixture * mixture, axis=0, keepdims=True) + 1e-05)
    hrow[...] = ((mixture * scale).T * gain[...]).astype(jnp.bfloat16).reshape(NY, ROWS, HEAD)

    def rows(k):
        return pl.ds(k * half, half)

    def h_copy(i, k, n, device):
        dst = hbuf.at[x, rows(k), pl.ds(pl.multiple_of(y * HEAD, HEAD), HEAD)]
        return rcopy(hrow.at[i, rows(k), :], dst, h_s.at[i, n], h_r.at[x, y, k], {"y": turn(i), **device})

    def h_arrived(xx, yy, k):
        dst = hbuf.at[xx, rows(k), pl.ds(pl.multiple_of(yy * HEAD, HEAD), HEAD)]
        rcopy(hrow.at[0, rows(k), :], dst, h_s.at[0, 0], h_r.at[xx, yy, k], {"x": right}).wait_recv()

    def h_relay(k):
        frm, to = ((left, right), (right, left))[k]
        ref = hbuf.at[frm, rows(k), :]
        return rcopy(ref, ref, hf_s.at[k], hf_r.at[k], {"x": to})

    sent = [h_copy(i, k, 4 + k, {}) for i in range(1, NY) for k in (0, 1)]
    for n, (k, to) in enumerate([(0, right), (1, left), (1, right), (0, left)]):
        sent += [h_copy(i, k, n, {"x": to}) for i in range(NY)]
    for copy in sent:
        copy.start()
    hbuf[x, :, mine] = hrow[0]
    for h in (0, 1):
        for k in range(1, NY):
            o_second(h, k).wait_send()
        for a in range(NY):
            for copy in o_third(h, a):
                copy.wait_send()
            for k in (0, 1):
                o_relay(h, a, k).wait_send()
            for b in range(NX):
                o_share(h, a, b).wait_send()
    for copy in own + [fwd_up, fwd_down]:
        copy.wait_send()
    ring.drain()
    for i in range(1, NY):
        for k in (0, 1):
            h_arrived(x, lax.rem(y + i, NY), k)

    depth = wt.shape[-1]

    def weights_here(xx):
        for h in (0, 1):
            for yy in range(NY):
                o_shared(h, *((yy, xx) if h == 0 else (xx, yy)))

    def product(xx):
        total = 0.0
        for h in (0, 1):
            total += lax.dot_general(
                wt[h, xx].reshape(-1, depth),
                hbuf[xx, :, h * depth : (h + 1) * depth],
                (((1,), (1,)), ((), ())),
                preferred_element_type=jnp.float32,
            )
        return total

    for xx in range(NX):
        weights_here(xx)
    osum[...] = product(x)
    relays = [h_relay(0), h_relay(1)]
    for k, frm in enumerate((left, right)):
        for i in range(NY):
            h_arrived(frm, lax.rem(y + i, NY), k)
        relays[k].start()
    for k, frm in enumerate((left, right)):
        for i in range(NY):
            h_arrived(frm, lax.rem(y + i, NY), 1 - k)
    osum[...] += product(left) + product(right)
    for k in (0, 1):
        ref = hbuf.at[facing, rows(k), :]
        rcopy(ref, ref, hf_s.at[k], hf_r.at[k], {"x": right}).wait_recv()
    out[...] = (osum[...] + product(facing)).astype(jnp.bfloat16).T

    for copy in sent + relays:
        copy.wait_send()


def attention(tokens, wq, wk, wv, wo, lam, gain):
    vmem = pl.BlockSpec(memory_space=pltpu.VMEM)
    dma = pltpu.SemaphoreType.DMA
    width = tokens.shape[1]
    w_sems, ring_sems = (
        [dma((2, NZ // 2, kinds)), dma((NZ, NC, kinds)), dma((NZ, kinds))] for kinds in (W_KINDS, KINDS)
    )
    return pl.pallas_call(
        attention_kernel,
        out_shape=jax.ShapeDtypeStruct(tokens.shape, jnp.bfloat16),
        in_specs=[vmem, vmem, vmem, vmem, vmem, pl.BlockSpec(memory_space=pltpu.SMEM), vmem],
        out_specs=vmem,
        scratch_shapes=[
            pltpu.VMEM((NY, ROWS, width), jnp.bfloat16),
            pltpu.VMEM((NZ, NY, NC, wq.shape[0], 2 * HEAD), jnp.bfloat16),
            pltpu.VMEM((NZ, NY, NC, wq.shape[0], HEAD), jnp.bfloat16),
            pltpu.VMEM((NZ, NC, TOKS, 2 * HEAD), jnp.bfloat16),
            pltpu.VMEM((TOKS, HEAD), jnp.bfloat16),
            pltpu.VMEM((HEAD, COLS), jnp.bfloat16),
            pltpu.VMEM((HEAD + 16, COLS), jnp.float32),
            pltpu.VMEM((8, COLS), jnp.float32),
            pltpu.VMEM((2, NX, NZ, NY, NC, wo.shape[0], wo.shape[1] // 2), jnp.bfloat16),
            pltpu.VMEM((NY, ROWS, HEAD), jnp.bfloat16),
            pltpu.VMEM((NX, ROWS, NY * HEAD), jnp.bfloat16),
            pltpu.VMEM((width, ROWS), jnp.float32),
            dma((6,)),
            dma((NY, 2)),
            dma((NY - 1, 3)),
            dma((NY, 3)),
            *w_sems,
            *ring_sems,
            dma((2, NY - 1)),
            dma((2, NY)),
            dma((2, NY, 4)),
            dma((2, NY, 2)),
            dma((2, NY, NX, 2)),
            dma((2, NY, NX)),
            dma((2, NY, NX)),
            dma((NY, 6)),
            dma((2,)),
            dma((NX, NY, 2)),
            dma((2,)),
        ],
        compiler_params=pltpu.CompilerParams(
            collective_id=0, has_side_effects=True, vmem_limit_bytes=56 * 1024 * 1024
        ),
        name="attention",
    )(tokens, wq, wk, wv, wo, lam, gain.reshape(1, -1))


def on_device(tokens, query_weight, key_weight, value_weight, out_weight, mix_lambda, head_gain):
    return attention(tokens, query_weight, key_weight, value_weight, out_weight.T, mix_lambda, head_gain)


def solution(mesh):
    fine = Mesh(mesh.devices.reshape(NZ, NY, NC, NX), ("z", "y", "core", "x"))
    sp = ("z", "y", "core")
    placed = (P(sp, None), P(sp, "x"), P(sp, "x"), P(sp, "x"), P("x", sp), P("x"), P())
    return jax.shard_map(on_device, mesh=fine, in_specs=placed, out_specs=P(sp, None), check_vma=False)
```

```python
import functools
import math

import jax
import jax.numpy as jnp
from jax import lax
from jax.experimental import pallas as pl
from jax.experimental.pallas import tpu as pltpu
from jax.sharding import Mesh
from jax.sharding import PartitionSpec as P

MESH = pl.DeviceIdType.MESH
NZ, NY, NC, NX = 8, 4, 2, 4
ROWS = 160
TOKS = NY * ROWS
HEAD = 128
COLS = 2 * TOKS
TILE = 256
KINDS = 4
LOW = -1e30
EXP_SCALE = 64 ** (-0.5) * math.log2(math.e)


def rcopy(src, dst, send_sem, recv_sem, device):
    return pltpu.make_async_remote_copy(
        src_ref=src, dst_ref=dst, send_sem=send_sem, recv_sem=recv_sem, device_id=device, device_id_type=MESH
    )


def attention_kernel(
    tok, wq, wk, wv, wo, lam, gain, out,
    xbuf, wkv, wqs, kv, qrow, qbd, acc, top, wt, hrow, hbuf, osum,
    send, tok_r, wy_r, wkv_r, wqs_r, wo_r, w_sib, kv_r, kv_sib, o2_r, o3_r, oc_r, h_r,
):
    z, y, c, x = (lax.axis_index(name) for name in ("z", "y", "core", "x"))
    right, left, facing = lax.rem(x + 1, NX), lax.rem(x + NX - 1, NX), lax.rem(x + 2, NX)
    above, below = lax.rem(y + 1, NY), lax.rem(y + NY - 1, NY)
    across = lax.rem(y + 2, NY)

    barrier = pltpu.get_barrier_semaphore()
    friends = [{"y": lax.rem(y + k, NY)} for k in range(1, NY)]
    friends += [{"z": lax.rem(z + k, NZ)} for k in range(1, NZ)]
    friends += [{"y": lax.rem(y + k, NY), "x": to} for k in range(NY) for to in (left, right)]
    friends += [{"x": facing}, {"core": 1 - c}]
    for friend in friends:
        pl.semaphore_signal(barrier, inc=1, device_id=friend, device_id_type=MESH)
    pl.semaphore_wait(barrier, len(friends))

    half = ROWS // 2

    SEND_TOK, SEND_WY, SEND_W, SEND_KV, SEND_O, SEND_SHARE, SEND_H = range(7)

    def wide(rows):
        return kv.at[pl.ds(0, rows), :]

    def got(sem, ref):
        rcopy(ref, ref, send.at[0], sem, {"core": 1 - c}).wait_recv()

    def gone(group, ref):
        rcopy(ref, ref, send.at[group], oc_r.at[0], {"core": 1 - c}).wait_send()

    def part(slot, k):
        return xbuf.at[slot, pl.ds(k * half, half), :]

    def tok_copy(src, slot, k, n, to):
        rcopy(src, part(slot, k), send.at[SEND_TOK], tok_r.at[n], {"y": to}).start()

    def w_slot(frm, n):
        return (wqs.at[z, frm, c], wkv.at[z, frm, c, :, pl.ds(0, HEAD)], wkv.at[z, frm, c, :, pl.ds(HEAD, HEAD)])[n]

    for n in (1, 2, 0):
        for k in range(1, NY):
            to = lax.rem(y + k, NY)
            src = (wq, wk, wv)[n].at[:, pl.ds(pl.multiple_of(to * HEAD, HEAD), HEAD)]
            rcopy(src, w_slot(y, n), send.at[SEND_WY], wy_r.at[min(n, 1)], {"y": to}).start()
    first_half, second_half = tok.at[pl.ds(0, half), :], tok.at[pl.ds(half, half), :]
    tok_copy(first_half, y, 0, 0, above)
    tok_copy(second_half, y, 1, 1, below)
    tok_copy(second_half, y, 1, 2, above)
    tok_copy(first_half, y, 0, 3, below)

    places = {"y": (y, above, below), "x": (x, right, left)}

    def axes(h):
        return ("y", "x") if h == 0 else ("x", "y")

    def piece(h, a, b, core, z_half=None):
        xx, yy = (b, a) if h == 0 else (a, b)
        zs = slice(None) if z_half is None else pl.ds(z_half * (NZ // 2), NZ // 2)
        return wt.at[h, xx, zs, yy, core]

    def turn(i, at=y):
        return lax.rem(at + jnp.where(i == 2, 3, jnp.where(i == 3, 2, i)), NY)

    def o_second(h, k):
        a, b = (places[name][0] for name in axes(h))
        ref = piece(h, a, b, c)
        to = {axes(h)[0]: lax.rem(a + k, NY)}
        rcopy(ref, ref, send.at[SEND_O], o2_r.at[h, k - 1], to).start()

    def o_share(h, a, b):
        ref = piece(h, a, b, c)
        rcopy(ref, ref, send.at[SEND_SHARE], oc_r.at[0], {"core": 1 - c}).start()

    def o_a(h, i):
        return lax.rem(places[axes(h)[0]][0] + (0, 3, 1, 2)[i], NY)

    def o_third(h, i):
        name = axes(h)[1]
        b, up, down = places[name]
        for k, to, group in [(0, up, 0), (1, down, 0), (1, up, 1), (0, down, 1)]:
            ref = piece(h, o_a(h, i), b, c, k)
            rcopy(ref, ref, send.at[SEND_O], o3_r.at[i, group], {name: to}).start()
        o_share(h, o_a(h, i), b)

    def o_relay(i):
        got(o3_r.at[i, 0], wide(512))
        for h in (1, 0):
            name = axes(h)[1]
            b, up, down = places[name]
            for k, (frm, to) in enumerate(((down, up), (up, down))):
                ref = piece(h, o_a(h, i), frm, c, k)
                rcopy(ref, ref, send.at[SEND_O], o3_r.at[i, 2], {name: to}).start()
        got(o3_r.at[i, 1], wide(512))
        for h in (1, 0):
            for frm in places[axes(h)[1]][1:]:
                o_share(h, o_a(h, i), frm)

    def o_last(i):
        got(o3_r.at[i, 2], wide(512))
        for h in (1, 0):
            o_share(h, o_a(h, i), lax.rem(places[axes(h)[1]][0] + 2, NY))

    def origin(way, d):
        return lax.rem(z + (NZ - d if way == 0 else d), NZ)

    def z_copy(ref, way, reach, group, sem):
        to = lax.rem(z + (reach if way == 0 else NZ - reach), NZ)
        rcopy(ref, ref, send.at[group], sem, {"z": to}).start()

    def share(ref, group, sem):
        rcopy(ref, ref, send.at[group], sem, {"core": 1 - c}).start()

    class Weights:
        def __init__(self, block, sem, sib):
            self.block, self.sem, self.sib = block, sem, sib

        def begin(self):
            for d in (2, 1):
                for kind in (0, 1):
                    for way in (0, 1):
                        z_copy(self.block(z, kind), way, d, SEND_W, self.sem(way, d, kind))
            self.to_sibling(z, (0, 1))

        def to_sibling(self, o, kinds):
            if self.sib is not None:
                for kind in kinds:
                    share(self.block(o, kind), SEND_W, self.sib)

        def pass_on(self, way, kinds):
            o = origin(way, 2)
            for kind in kinds:
                z_copy(self.block(o, kind), way, 1, SEND_W, self.sem(way, 3, kind))
                if way == kind:
                    z_copy(self.block(o, kind), way, 2, SEND_W, self.sem(way, 4, kind))
            self.to_sibling(o, kinds)

        def arrived(self, d):
            for way in (0, 1):
                self.to_sibling(origin(way, d), (0, 1) if d < 4 else (way,))

    key_value = Weights(
        lambda o, kind: wkv.at[o, pl.ds(2 * kind, 2), c],
        lambda way, d, kind: wkv_r.at[2 * way + kind if d == 2 else {1: 4, 4: 5, 3: 6}[d]],
        w_sib.at[0],
    )
    query = Weights(
        lambda o, kind: wqs.at[o, pl.ds(2 * kind, 2), c],
        lambda way, d, kind: wqs_r.at[way if d == 2 else 2],
        w_sib.at[1],
    )
    output = Weights(
        lambda o, kind: wt.at[kind, x, o, y, c], lambda way, d, kind: wo_r.at[way if d == 2 else 2], None
    )

    def kv_block(o, cc, kind):
        return kv.at[pl.ds(pl.multiple_of(((o * NC + cc) * KINDS + kind) * ROWS, ROWS), ROWS), :]

    def farthest(way, kind):
        return NZ // 2 - (way != kind % 2)

    def kv_begin(kind):
        for way in (0, 1):
            z_copy(kv_block(z, c, kind), way, 1, SEND_KV, kv_r.at[way, 0, kind])
        share(kv_block(z, c, kind), SEND_KV, kv_sib.at[z])

    def kv_pass(way, d, kind):
        o = origin(way, d)
        got(kv_r.at[way, d - 1, kind], wide(ROWS))

        @pl.when(d < farthest(way, kind))
        def _():
            z_copy(kv_block(o, c, kind), way, 1, SEND_KV, kv_r.at[way, d, kind])

        share(kv_block(o, c, kind), SEND_KV, kv_sib.at[o])

    for h in (0, 1):
        wt[h, x, z, y, c] = wo[:, h * wo.shape[1] // 2 : (h + 1) * wo.shape[1] // 2]
    output.begin()

    mine = pl.ds(pl.multiple_of(y * HEAD, HEAD), HEAD)
    wqs[z, y, c] = wq[:, mine]
    wkv[z, y, c, :, :HEAD] = wk[:, mine]
    wkv[z, y, c, :, HEAD:] = wv[:, mine]
    xbuf[y] = tok[...]
    acc[...] = jnp.zeros_like(acc)
    top[...] = jnp.full_like(top, LOW)

    got(wy_r.at[1], wide(3 * 32))
    key_value.begin()
    for kind in (0, 1):
        for way in (0, 1):
            got(wkv_r.at[2 * way + kind], wide(64))
            key_value.pass_on(way, (kind,))
    for way in (0, 1):
        got(wo_r.at[way], wide(64))
        output.pass_on(way, (0, 1))
    got(wy_r.at[0], qrow.at[pl.ds(0, 3 * 32), :])
    query.begin()
    got(wkv_r.at[4], wide(256))
    key_value.arrived(1)
    got(tok_r.at[0], part(below, 0))
    tok_copy(part(below, 0), below, 0, 4, above)
    got(tok_r.at[1], part(above, 1))
    tok_copy(part(above, 1), above, 1, 4, below)
    for way in (0, 1):
        got(wqs_r.at[way], wide(64))
        query.pass_on(way, (0, 1))
    got(wkv_r.at[6], wide(256))
    key_value.arrived(3)
    got(wkv_r.at[5], wide(128))
    key_value.arrived(4)
    got(w_sib.at[0], wide(NZ * NY * 32))

    def project(i):
        kv_block(z, c, i)[...] = jnp.dot(
            xbuf[turn(i)], wkv[...].reshape(-1, 2 * HEAD), preferred_element_type=jnp.float32
        ).astype(jnp.bfloat16)
        kv_begin(i)

    def project_near(i, carry):
        @pl.when(i == 1)
        def _():
            got(tok_r.at[3], part(above, 0))

        @pl.when(i == 2)
        def _():
            got(tok_r.at[2], part(below, 1))

        project(i)
        return carry

    lax.fori_loop(0, NY - 1, project_near, 0)

    got(wo_r.at[2], wide(10 * 32))
    for h in (1, 0):
        for k in (1, 3, 2):
            o_second(h, k)
        o_third(h, 0)
    got(wqs_r.at[2], wide(10 * 32))
    for d in (1, 3, 4):
        query.arrived(d)
    gone(SEND_WY, qrow.at[pl.ds(0, 9 * 32), :])
    gone(SEND_W, wide(30 * 64 + 30 * 32 + 14 * 32))
    got(tok_r.at[4], xbuf.at[across])
    project(NY - 1)
    for kind in range(NY - 1):
        for way in (0, 1):
            kv_pass(way, 1, kind)
    got(w_sib.at[1], wide(NZ * NY * 16))

    def queries(i, carry):
        at = pl.ds(pl.multiple_of(i * ROWS, ROWS), ROWS)
        qrow[at, :] = jnp.dot(
            xbuf[turn(i)], wqs[...].reshape(-1, HEAD), preferred_element_type=jnp.float32
        ).astype(jnp.bfloat16)
        return carry

    lax.fori_loop(0, NY, queries, 0)
    q_t = qrow[...].T
    first = lax.broadcasted_iota(jnp.int32, q_t.shape, 0) < HEAD // 2
    zero = jnp.zeros_like(q_t)
    qbd[:, :TOKS] = jnp.where(first, q_t, zero)
    qbd[:, TOKS:] = jnp.where(first, zero, q_t)

    ones = jnp.ones((16, TOKS), jnp.bfloat16)

    def place(r, core):
        i = sum((r >= k * ROWS).astype(jnp.int32) for k in range(1, NY))
        return r + ROWS * (2 * turn(i) - i + core)

    def visit(o, cc, masked):
        at = pl.ds(pl.multiple_of((o * NC + cc) * TOKS, TOKS), TOKS)
        keys = kv[at, :HEAD]
        values = jnp.concatenate([kv[at, HEAD:].T, ones], axis=0)

        def scores(j):
            return jnp.dot(keys, qbd[:, j * TILE : (j + 1) * TILE], preferred_element_type=jnp.float32)

        ahead = scores(0)
        for j in range(COLS // TILE):
            cols = slice(j * TILE, (j + 1) * TILE)
            s = ahead
            if j + 1 < COLS // TILE:
                ahead = scores(j + 1)
            if masked:
                u = lax.broadcasted_iota(jnp.int32, (TOKS, 1), 0)
                t = lax.broadcasted_iota(jnp.int32, (1, TILE), 1) + j * TILE
                t = jnp.where(t >= TOKS, t - TOKS, t)
                s = jnp.where(place(u, cc) <= place(t, c), s, LOW)
            before = top[0:1, cols]
            now = jnp.maximum(before, jnp.max(s, axis=0, keepdims=True))
            shrink = jnp.exp2((before - now) * EXP_SCALE)
            p = jnp.exp2((s - now) * EXP_SCALE).astype(jnp.bfloat16)
            acc[:, cols] = acc[:, cols] * shrink + jnp.dot(values, p, preferred_element_type=jnp.float32)
            top[0:1, cols] = now

    def own_slice(k, carry):
        cc = jnp.where(k == 0, c, 1 - c)

        @pl.when(k == 1)
        def _():
            got(kv_sib.at[z], wide(TOKS))

        visit(z, cc, True)
        return carry

    lax.fori_loop(0, NC, own_slice, 0)

    def step(d, carry):
        for way in (0, 1):
            for kind in (2 * way, 2 * way + 1):
                for course in (0, 1):
                    due = d <= farthest(course, kind)

                    @pl.when(due if kind == KINDS - 1 else due & (d > 1))
                    def _():
                        kv_pass(course, d, kind)

            before = d - 1
            o = origin(way, before)
            there = (before >= 1) & (before <= NZ // 2 - way)

            @pl.when(there)
            def _():
                got(kv_sib.at[o], wide(TOKS))

            @pl.when(there & (o < z))
            def _():
                def both(cc, carry):
                    visit(o, cc, False)
                    return carry

                lax.fori_loop(0, NC, both, 0)

        @pl.when(d == 1)
        def _():
            for i, k in ((1, 1), (2, 3), (3, 2)):
                for h in (1, 0):
                    got(o2_r.at[h, k - 1], wide(256))
                    o_third(h, i)

        for i, at in enumerate((1, 2, 3, 3)):

            @pl.when(d == at)
            def _():
                o_relay(i)

            @pl.when(d == (4 if i < 2 else 5))
            def _():
                o_last(i)

        return carry

    lax.fori_loop(1, NZ // 2 + 2, step, 0)

    def part_of(cols):
        return acc[:HEAD, cols] / acc[HEAD : HEAD + 1, cols]

    mixture = part_of(slice(0, TOKS)) - lam[y] * part_of(slice(TOKS, COLS))
    scale = lax.rsqrt(jnp.mean(mixture * mixture, axis=0, keepdims=True) + 1e-05)
    hrow[...] = ((mixture * scale).T * gain[...]).astype(jnp.bfloat16).reshape(NY, ROWS, HEAD)

    def rows(k):
        return pl.ds(k * half, half)

    def h_copy(i, k, sem, device):
        dst = hbuf.at[x, rows(k), pl.ds(pl.multiple_of(y * HEAD, HEAD), HEAD)]
        rcopy(hrow.at[i, rows(k), :], dst, send.at[SEND_H], h_r.at[sem], {"y": turn(i), **device}).start()

    for i in range(1, NY):
        for k in (0, 1):
            h_copy(i, k, 0, {})
    for k, to, sem in [(0, right, 1), (1, left, 2), (1, right, 3), (0, left, 3)]:
        for i in range(NY):
            h_copy(i, k, sem, {"x": to})
    hbuf[x, :, mine] = hrow[0]
    gone(SEND_O, wide(6 * 256 + 48 * 128))
    gone(SEND_SHARE, wt.at[0])
    gone(SEND_TOK, xbuf.at[pl.ds(0, 3)])
    gone(SEND_KV, wide(60 * ROWS))
    got(h_r.at[0], wide(3 * half))

    depth = wt.shape[-1]

    def product(xx):
        total = 0.0
        for h in (0, 1):
            total += lax.dot_general(
                wt[h, xx].reshape(-1, depth),
                hbuf[xx, :, h * depth : (h + 1) * depth],
                (((1,), (1,)), ((), ())),
                preferred_element_type=jnp.float32,
            )
        return total

    got(oc_r.at[0], wt.at[0])
    osum[...] = product(x)
    for k, (frm, to) in enumerate(((left, right), (right, left))):
        got(h_r.at[1 + k], wide(2 * half))
        ref = hbuf.at[frm, rows(k), :]
        rcopy(ref, ref, send.at[SEND_H], h_r.at[4], {"x": to}).start()
    got(h_r.at[3], wide(4 * half))
    osum[...] += product(left) + product(right)
    got(h_r.at[4], wide(4 * half))
    out[...] = (osum[...] + product(facing)).astype(jnp.bfloat16).T

    gone(SEND_H, wide(22 * half // 2 + 4 * half))


def attention(tokens, wq, wk, wv, wo, lam, gain):
    vmem = pl.BlockSpec(memory_space=pltpu.VMEM)
    dma = pltpu.SemaphoreType.DMA
    width = tokens.shape[1]
    return pl.pallas_call(
        attention_kernel,
        out_shape=jax.ShapeDtypeStruct(tokens.shape, jnp.bfloat16),
        in_specs=[vmem, vmem, vmem, vmem, vmem, pl.BlockSpec(memory_space=pltpu.SMEM), vmem],
        out_specs=vmem,
        scratch_shapes=[
            pltpu.VMEM((NY, ROWS, width), jnp.bfloat16),
            pltpu.VMEM((NZ, NY, NC, wq.shape[0], 2 * HEAD), jnp.bfloat16),
            pltpu.VMEM((NZ, NY, NC, wq.shape[0], HEAD), jnp.bfloat16),
            pltpu.VMEM((NZ * NC * TOKS, 2 * HEAD), jnp.bfloat16),
            pltpu.VMEM((TOKS, HEAD), jnp.bfloat16),
            pltpu.VMEM((HEAD, COLS), jnp.bfloat16),
            pltpu.VMEM((HEAD + 16, COLS), jnp.float32),
            pltpu.VMEM((8, COLS), jnp.float32),
            pltpu.VMEM((2, NX, NZ, NY, NC, wo.shape[0], wo.shape[1] // 2), jnp.bfloat16),
            pltpu.VMEM((NY, ROWS, HEAD), jnp.bfloat16),
            pltpu.VMEM((NX, ROWS, NY * HEAD), jnp.bfloat16),
            pltpu.VMEM((width, ROWS), jnp.float32),
            dma((7,)),
            dma((5,)),
            dma((2,)),
            dma((7,)),
            dma((3,)),
            dma((3,)),
            dma((2,)),
            dma((2, NZ // 2, KINDS)),
            dma((NZ,)),
            dma((2, NY - 1)),
            dma((NY, 3)),
            dma((1,)),
            dma((5,)),
        ],
        compiler_params=pltpu.CompilerParams(
            collective_id=0, has_side_effects=True, vmem_limit_bytes=56 * 1024 * 1024
        ),
        name="attention",
    )(tokens, wq, wk, wv, wo, lam, gain.reshape(1, -1))


def on_device(tokens, query_weight, key_weight, value_weight, out_weight, mix_lambda, head_gain):
    return attention(tokens, query_weight, key_weight, value_weight, out_weight.T, mix_lambda, head_gain)


def solution(mesh):
    fine = Mesh(mesh.devices.reshape(NZ, NY, NC, NX), ("z", "y", "core", "x"))
    sp = ("z", "y", "core")
    placed = (P(sp, None), P(sp, "x"), P(sp, "x"), P(sp, "x"), P("x", sp), P("x"), P())
    return jax.shard_map(on_device, mesh=fine, in_specs=placed, out_specs=P(sp, None), check_vma=False)
```

```python
import functools
import math

import jax
import jax.numpy as jnp
from jax import lax
from jax.experimental import pallas as pl
from jax.experimental.pallas import tpu as pltpu
from jax.sharding import Mesh
from jax.sharding import PartitionSpec as P

MESH = pl.DeviceIdType.MESH
NZ, NY, NC, NX = 8, 4, 2, 4
ROWS = 160
TOKS = NY * ROWS
HEAD = 128
COLS = 2 * TOKS
TILE = 256
KINDS = 4
LOW = -1e30
EXP_SCALE = 64 ** (-0.5) * math.log2(math.e)


def rcopy(src, dst, send_sem, recv_sem, device):
    return pltpu.make_async_remote_copy(
        src_ref=src, dst_ref=dst, send_sem=send_sem, recv_sem=recv_sem, device_id=device, device_id_type=MESH
    )


def attention_kernel(
    tok, wq, wk, wv, wo, lam, gain, out,
    xbuf, wloc, wkv, wqs, kv, qrow, qbd, acc, top, wt, hrow, hbuf, osum,
    into, send, tok_r, wy_r, wkv_r, wqs_r, wo_r, w_sib, kv_r, kv_sib, o2_r, o3_r, oc_r, h_r,
):
    z, y, c, x = (lax.axis_index(name) for name in ("z", "y", "core", "x"))
    right, left, facing = lax.rem(x + 1, NX), lax.rem(x + NX - 1, NX), lax.rem(x + 2, NX)
    above, below = lax.rem(y + 1, NY), lax.rem(y + NY - 1, NY)
    across = lax.rem(y + 2, NY)

    inputs = [
        pltpu.make_async_copy(src, dst, into.at[n])
        for n, (src, dst) in enumerate(
            [(wk, wloc.at[1]), (wv, wloc.at[2]), (wq, wloc.at[0]), (tok, xbuf.at[y]), (wo, wt.at[x, z, y, c])]
        )
    ]
    for copy in inputs:
        copy.start()

    barrier = pltpu.get_barrier_semaphore()
    friends = [{"y": lax.rem(y + k, NY)} for k in range(1, NY)]
    friends += [{"z": lax.rem(z + k, NZ)} for k in range(1, NZ)]
    friends += [{"y": lax.rem(y + k, NY), "x": to} for k in range(NY) for to in (left, right)]
    friends += [{"x": facing}, {"core": 1 - c}]
    for friend in friends:
        pl.semaphore_signal(barrier, inc=1, device_id=friend, device_id_type=MESH)
    for copy in inputs:
        copy.wait()
    pl.semaphore_wait(barrier, len(friends))

    half = ROWS // 2

    SEND_TOK, SEND_WY, SEND_W, SEND_KV, SEND_O, SEND_SHARE, SEND_H = range(7)

    def wide(rows):
        return kv.at[pl.ds(0, rows), :]

    def got(sem, ref):
        rcopy(ref, ref, send.at[0], sem, {"core": 1 - c}).wait_recv()

    def gone(group, ref):
        rcopy(ref, ref, send.at[group], oc_r.at[0], {"core": 1 - c}).wait_send()

    share_of = xbuf.shape[2] // 4
    near = pl.ds(pl.multiple_of(lax.rem(x, 2) * share_of, share_of), 3 * share_of)
    missed = pl.ds(pl.multiple_of(lax.rem(x, 2) * 3 * share_of, share_of), share_of)

    def part(slot, k, lanes=near):
        return xbuf.at[slot, pl.ds(k * half, half), lanes]

    def tok_copy(slot, k, n, to):
        rcopy(part(slot, k), part(slot, k), send.at[SEND_TOK], tok_r.at[n], {"y": to}).start()

    def tok_aside(slot, k, n):
        ref = part(slot, k, missed)
        rcopy(ref, ref, send.at[SEND_TOK], tok_r.at[n], {"x": (right, left)[k]}).start()

    def tok_complete(slot, n):
        got(tok_r.at[n], xbuf.at[slot, :, pl.ds(0, share_of)])

    def w_slot(frm, n):
        return (wqs.at[z, frm, c], wkv.at[z, frm, c, :, pl.ds(0, HEAD)], wkv.at[z, frm, c, :, pl.ds(HEAD, HEAD)])[n]

    for n in (1, 2, 0):
        for k in range(1, NY):
            to = lax.rem(y + k, NY)
            src = wloc.at[n, :, pl.ds(pl.multiple_of(to * HEAD, HEAD), HEAD)]
            rcopy(src, w_slot(y, n), send.at[SEND_WY], wy_r.at[min(n, 1)], {"y": to}).start()
    tok_copy(y, 0, 0, above)
    tok_copy(y, 1, 1, below)
    tok_copy(y, 1, 2, above)
    tok_copy(y, 0, 3, below)

    depth = wo.shape[1] // 2
    places = {"y": (y, above, below), "x": (x, right, left)}

    def axes(h):
        return ("y", "x") if h == 0 else ("x", "y")

    def piece(h, a, b, core, z_half=None):
        xx, yy = (b, a) if h == 0 else (a, b)
        zs = slice(None) if z_half is None else pl.ds(z_half * (NZ // 2), NZ // 2)
        return wt.at[xx, zs, yy, core, :, pl.ds(h * depth, depth)]

    def turn(i, at=y):
        return lax.rem(at + jnp.where(i == 2, 3, jnp.where(i == 3, 2, i)), NY)

    def o_second(h, k):
        a, b = (places[name][0] for name in axes(h))
        ref = piece(h, a, b, c)
        to = {axes(h)[0]: lax.rem(a + k, NY)}
        rcopy(ref, ref, send.at[SEND_O], o2_r.at[h, k - 1], to).start()

    def o_share(h, a, b):
        ref = piece(h, a, b, c)
        rcopy(ref, ref, send.at[SEND_SHARE], oc_r.at[0], {"core": 1 - c}).start()

    def o_a(h, i):
        return lax.rem(places[axes(h)[0]][0] + (0, 3, 1, 2)[i], NY)

    def o_third(h, i):
        name = axes(h)[1]
        b, up, down = places[name]
        for k, to, group in [(0, up, 0), (1, down, 0), (1, up, 1), (0, down, 1)]:
            ref = piece(h, o_a(h, i), b, c, k)
            rcopy(ref, ref, send.at[SEND_O], o3_r.at[i, group], {name: to}).start()
        o_share(h, o_a(h, i), b)

    def o_relay(i):
        got(o3_r.at[i, 0], wide(512))
        for h in (1, 0):
            name = axes(h)[1]
            b, up, down = places[name]
            for k, (frm, to) in enumerate(((down, up), (up, down))):
                ref = piece(h, o_a(h, i), frm, c, k)
                rcopy(ref, ref, send.at[SEND_O], o3_r.at[i, 2], {name: to}).start()
        got(o3_r.at[i, 1], wide(512))
        for h in (1, 0):
            for frm in places[axes(h)[1]][1:]:
                o_share(h, o_a(h, i), frm)

    def o_last(i):
        got(o3_r.at[i, 2], wide(512))
        for h in (1, 0):
            o_share(h, o_a(h, i), lax.rem(places[axes(h)[1]][0] + 2, NY))

    def origin(way, d):
        return lax.rem(z + (NZ - d if way == 0 else d), NZ)

    def z_copy(ref, way, reach, group, sem):
        to = lax.rem(z + (reach if way == 0 else NZ - reach), NZ)
        rcopy(ref, ref, send.at[group], sem, {"z": to}).start()

    def share(ref, group, sem):
        rcopy(ref, ref, send.at[group], sem, {"core": 1 - c}).start()

    class Weights:
        def __init__(self, block, sem, sib):
            self.block, self.sem, self.sib = block, sem, sib

        def begin(self):
            for d in (2, 1):
                for kind in (0, 1):
                    for way in (0, 1):
                        z_copy(self.block(z, kind), way, d, SEND_W, self.sem(way, d, kind))
            self.to_sibling(z, (0, 1))

        def to_sibling(self, o, kinds):
            if self.sib is not None:
                for kind in kinds:
                    share(self.block(o, kind), SEND_W, self.sib)

        def pass_on(self, way, kinds):
            o = origin(way, 2)
            for kind in kinds:
                z_copy(self.block(o, kind), way, 1, SEND_W, self.sem(way, 3, kind))
                if way == kind:
                    z_copy(self.block(o, kind), way, 2, SEND_W, self.sem(way, 4, kind))
            self.to_sibling(o, kinds)

        def arrived(self, d):
            for way in (0, 1):
                self.to_sibling(origin(way, d), (0, 1) if d < 4 else (way,))

    key_value = Weights(
        lambda o, kind: wkv.at[o, pl.ds(2 * kind, 2), c],
        lambda way, d, kind: wkv_r.at[2 * way + kind if d == 2 else {1: 4, 4: 5, 3: 6}[d]],
        w_sib.at[0],
    )
    query = Weights(
        lambda o, kind: wqs.at[o, pl.ds(2 * kind, 2), c],
        lambda way, d, kind: wqs_r.at[way if d == 2 else 2],
        w_sib.at[1],
    )
    output = Weights(
        lambda o, kind: wt.at[x, o, y, c, :, pl.ds(kind * depth, depth)], lambda way, d, kind: wo_r.at[way if d == 2 else 2], None
    )

    def kv_block(o, cc, kind):
        return kv.at[pl.ds(pl.multiple_of(((o * NC + cc) * KINDS + kind) * ROWS, ROWS), ROWS), :]

    def farthest(way, kind):
        return NZ // 2 - (way != kind % 2)

    def kv_begin(kind):
        for way in (0, 1):
            z_copy(kv_block(z, c, kind), way, 1, SEND_KV, kv_r.at[way, 0, kind])
        share(kv_block(z, c, kind), SEND_KV, kv_sib.at[z])

    def kv_pass(way, d, kind):
        o = origin(way, d)
        got(kv_r.at[way, d - 1, kind], wide(ROWS))

        @pl.when(d < farthest(way, kind))
        def _():
            z_copy(kv_block(o, c, kind), way, 1, SEND_KV, kv_r.at[way, d, kind])

        share(kv_block(o, c, kind), SEND_KV, kv_sib.at[o])

    output.begin()

    mine = pl.ds(pl.multiple_of(y * HEAD, HEAD), HEAD)
    wqs[z, y, c] = wloc[0, :, mine]
    wkv[z, y, c, :, :HEAD] = wloc[1, :, mine]
    wkv[z, y, c, :, HEAD:] = wloc[2, :, mine]
    acc[...] = jnp.zeros_like(acc)
    top[...] = jnp.full_like(top, LOW)

    got(wy_r.at[1], wide(3 * 32))
    key_value.begin()
    for kind in (0, 1):
        for way in (0, 1):
            got(wkv_r.at[2 * way + kind], wide(64))
            key_value.pass_on(way, (kind,))
    for way in (0, 1):
        got(wo_r.at[way], wide(64))
        output.pass_on(way, (0, 1))
    got(wy_r.at[0], qrow.at[pl.ds(0, 3 * 32), :])
    query.begin()
    got(wkv_r.at[4], wide(256))
    key_value.arrived(1)
    got(tok_r.at[0], part(below, 0))
    tok_copy(below, 0, 4, above)
    tok_aside(below, 0, 6)
    got(tok_r.at[1], part(above, 1))
    tok_copy(above, 1, 4, below)
    tok_aside(above, 1, 5)
    got(wkv_r.at[6], wide(256))
    key_value.arrived(3)
    got(wkv_r.at[5], wide(128))
    key_value.arrived(4)
    for way in (0, 1):
        got(wqs_r.at[way], wide(64))
        query.pass_on(way, (0, 1))
    got(tok_r.at[2], part(below, 1))
    tok_aside(below, 1, 6)
    got(tok_r.at[3], part(above, 0))
    tok_aside(above, 0, 5)
    got(w_sib.at[0], wide(NZ * NY * 32))

    def project(i):
        kv_block(z, c, i)[...] = jnp.dot(
            xbuf[turn(i)], wkv[...].reshape(-1, 2 * HEAD), preferred_element_type=jnp.float32
        ).astype(jnp.bfloat16)
        kv_begin(i)

    def project_near(i, carry):
        @pl.when(i == 1)
        def _():
            tok_complete(above, 5)

        @pl.when(i == 2)
        def _():
            tok_complete(below, 6)

        project(i)
        return carry

    lax.fori_loop(0, NY - 1, project_near, 0)

    got(tok_r.at[4], xbuf.at[across, :, near])
    for k in (0, 1):
        tok_aside(across, k, 7)
    got(wo_r.at[2], wide(10 * 32))
    for h in (1, 0):
        for k in (1, 3, 2):
            o_second(h, k)
        o_third(h, 0)
    got(wqs_r.at[2], wide(10 * 32))
    for d in (1, 3, 4):
        query.arrived(d)
    gone(SEND_WY, qrow.at[pl.ds(0, 9 * 32), :])
    gone(SEND_W, wide(30 * 64 + 30 * 32 + 14 * 32))
    tok_complete(across, 7)
    project(NY - 1)
    for kind in range(NY - 1):
        for way in (0, 1):
            kv_pass(way, 1, kind)
    got(w_sib.at[1], wide(NZ * NY * 16))

    def queries(i, carry):
        at = pl.ds(pl.multiple_of(i * ROWS, ROWS), ROWS)
        qrow[at, :] = jnp.dot(
            xbuf[turn(i)], wqs[...].reshape(-1, HEAD), preferred_element_type=jnp.float32
        ).astype(jnp.bfloat16)
        return carry

    lax.fori_loop(0, NY, queries, 0)
    q_t = qrow[...].T
    first = lax.broadcasted_iota(jnp.int32, q_t.shape, 0) < HEAD // 2
    zero = jnp.zeros_like(q_t)
    qbd[:, :TOKS] = jnp.where(first, q_t, zero)
    qbd[:, TOKS:] = jnp.where(first, zero, q_t)

    ones = jnp.ones((16, NC * TOKS), jnp.bfloat16)

    def place(r, core):
        i = sum((r >= k * ROWS).astype(jnp.int32) for k in range(1, NY))
        return r + ROWS * (2 * turn(i) - i + core)

    def visit(o, masked):
        at = pl.ds(pl.multiple_of(o * NC * TOKS, NC * TOKS), NC * TOKS)
        keys = kv[at, :HEAD]
        values = jnp.concatenate([kv[at, HEAD:].T, ones], axis=0)

        def scores(j):
            return jnp.dot(keys, qbd[:, j * TILE : (j + 1) * TILE], preferred_element_type=jnp.float32)

        ahead = scores(0)
        for j in range(COLS // TILE):
            cols = slice(j * TILE, (j + 1) * TILE)
            s = ahead
            if j + 1 < COLS // TILE:
                ahead = scores(j + 1)
            if masked:
                u = lax.broadcasted_iota(jnp.int32, (NC * TOKS, 1), 0)
                core = (u >= TOKS).astype(jnp.int32)
                t = lax.broadcasted_iota(jnp.int32, (1, TILE), 1) + j * TILE
                t = jnp.where(t >= TOKS, t - TOKS, t)
                s = jnp.where(place(u - TOKS * core, core) <= place(t, c), s, LOW)
            before = top[0:1, cols]
            now = jnp.maximum(before, jnp.max(s, axis=0, keepdims=True))
            shrink = jnp.exp2((before - now) * EXP_SCALE)
            p = jnp.exp2((s - now) * EXP_SCALE).astype(jnp.bfloat16)
            acc[:, cols] = acc[:, cols] * shrink + jnp.dot(values, p, preferred_element_type=jnp.float32)
            top[0:1, cols] = now

    got(kv_sib.at[z], wide(TOKS))
    visit(z, True)

    def pieces_on(h):
        for i, k in ((1, 1), (2, 3), (3, 2)):
            got(o2_r.at[h, k - 1], wide(256))
            o_third(h, i)

    def step(d, carry):
        for way in (0, 1):
            for kind in (2 * way, 2 * way + 1):
                for course in (0, 1):
                    due = d <= farthest(course, kind)

                    @pl.when(due if kind == KINDS - 1 else due & (d > 1))
                    def _():
                        kv_pass(course, d, kind)

            before = d - 1
            o = origin(way, before)
            there = (before >= 1) & (before <= NZ // 2 - way)

            @pl.when(there)
            def _():
                got(kv_sib.at[o], wide(TOKS))

            @pl.when(there & (o < z))
            def _():
                visit(o, False)

            if way == 0:

                @pl.when(d == 2)
                def _():
                    pieces_on(0)

        @pl.when(d == 1)
        def _():
            pieces_on(1)

        for i, at in enumerate((2, 3, 4, 4)):

            @pl.when(d == at)
            def _():
                o_relay(i)

        return carry

    lax.fori_loop(1, NZ // 2 + 2, step, 0)

    def part_of(cols):
        return acc[:HEAD, cols] / acc[HEAD : HEAD + 1, cols]

    mixture = part_of(slice(0, TOKS)) - lam[y] * part_of(slice(TOKS, COLS))
    scale = lax.rsqrt(jnp.mean(mixture * mixture, axis=0, keepdims=True) + 1e-05)
    hrow[...] = ((mixture * scale).T * gain[...]).astype(jnp.bfloat16).reshape(NY, ROWS, HEAD)

    def rows(k):
        return pl.ds(k * half, half)

    def h_copy(i, k, sem, device):
        dst = hbuf.at[x, rows(k), pl.ds(pl.multiple_of(y * HEAD, HEAD), HEAD)]
        rcopy(hrow.at[i, rows(k), :], dst, send.at[SEND_H], h_r.at[sem], {"y": turn(i), **device}).start()

    for i in range(1, NY):
        for k in (0, 1):
            h_copy(i, k, 0, {})
    for k, to, sem in [(0, right, 1), (1, left, 2), (1, right, 3), (0, left, 3)]:
        for i in range(NY):
            h_copy(i, k, sem, {"x": to})
    hbuf[x, :, mine] = hrow[0]
    for i in range(NY):
        o_last(i)
    for k, (frm, to) in enumerate(((left, right), (right, left))):
        got(h_r.at[1 + k], wide(2 * half))
        ref = hbuf.at[frm, rows(k), :]
        rcopy(ref, ref, send.at[SEND_H], h_r.at[4], {"x": to}).start()
    got(h_r.at[0], wide(3 * half))

    def product(xx):
        return lax.dot_general(
            wt[xx].reshape(-1, wo.shape[1]),
            hbuf[xx],
            (((1,), (1,)), ((), ())),
            preferred_element_type=jnp.float32,
        )

    got(oc_r.at[0], wt.at[pl.ds(0, 2)])
    osum[...] = product(x)
    gone(SEND_O, wide(6 * 256 + 48 * 128))
    gone(SEND_SHARE, wt.at[pl.ds(0, 2)])
    gone(SEND_TOK, xbuf.at[pl.ds(0, 3)])
    gone(SEND_KV, wide(60 * ROWS))
    got(h_r.at[3], wide(4 * half))
    osum[...] += product(left) + product(right)
    got(h_r.at[4], wide(4 * half))
    out[...] = (osum[...] + product(facing)).astype(jnp.bfloat16).T

    gone(SEND_H, wide(22 * half // 2 + 4 * half))


def attention(tokens, wq, wk, wv, wo, lam, gain):
    vmem = pl.BlockSpec(memory_space=pltpu.VMEM)
    hbm = pl.BlockSpec(memory_space=pltpu.HBM)
    dma = pltpu.SemaphoreType.DMA
    width = tokens.shape[1]
    return pl.pallas_call(
        attention_kernel,
        out_shape=jax.ShapeDtypeStruct(tokens.shape, jnp.bfloat16),
        in_specs=[hbm, hbm, hbm, hbm, hbm, pl.BlockSpec(memory_space=pltpu.SMEM), vmem],
        out_specs=vmem,
        scratch_shapes=[
            pltpu.VMEM((NY, ROWS, width), jnp.bfloat16),
            pltpu.VMEM((3, *wq.shape), jnp.bfloat16),
            pltpu.VMEM((NZ, NY, NC, wq.shape[0], 2 * HEAD), jnp.bfloat16),
            pltpu.VMEM((NZ, NY, NC, wq.shape[0], HEAD), jnp.bfloat16),
            pltpu.VMEM((NZ * NC * TOKS, 2 * HEAD), jnp.bfloat16),
            pltpu.VMEM((TOKS, HEAD), jnp.bfloat16),
            pltpu.VMEM((HEAD, COLS), jnp.bfloat16),
            pltpu.VMEM((HEAD + 16, COLS), jnp.float32),
            pltpu.VMEM((8, COLS), jnp.float32),
            pltpu.VMEM((NX, NZ, NY, NC, wo.shape[0], wo.shape[1]), jnp.bfloat16),
            pltpu.VMEM((NY, ROWS, HEAD), jnp.bfloat16),
            pltpu.VMEM((NX, ROWS, NY * HEAD), jnp.bfloat16),
            pltpu.VMEM((width, ROWS), jnp.float32),
            dma((5,)),
            dma((7,)),
            dma((8,)),
            dma((2,)),
            dma((7,)),
            dma((3,)),
            dma((3,)),
            dma((2,)),
            dma((2, NZ // 2, KINDS)),
            dma((NZ,)),
            dma((2, NY - 1)),
            dma((NY, 3)),
            dma((1,)),
            dma((5,)),
        ],
        compiler_params=pltpu.CompilerParams(
            collective_id=0, has_side_effects=True, vmem_limit_bytes=56 * 1024 * 1024
        ),
        name="attention",
    )(tokens, wq, wk, wv, wo, lam, gain.reshape(1, -1))


def on_device(tokens, query_weight, key_weight, value_weight, out_weight, mix_lambda, head_gain):
    return attention(tokens, query_weight, key_weight, value_weight, out_weight.T, mix_lambda, head_gain)


def solution(mesh):
    fine = Mesh(mesh.devices.reshape(NZ, NY, NC, NX), ("z", "y", "core", "x"))
    sp = ("z", "y", "core")
    placed = (P(sp, None), P(sp, "x"), P(sp, "x"), P(sp, "x"), P("x", sp), P("x"), P())
    return jax.shard_map(on_device, mesh=fine, in_specs=placed, out_specs=P(sp, None), check_vma=False)
```

```python
import functools
import math

import jax
import jax.numpy as jnp
from jax import lax
from jax.experimental import pallas as pl
from jax.experimental.pallas import tpu as pltpu
from jax.sharding import Mesh
from jax.sharding import PartitionSpec as P

MESH = pl.DeviceIdType.MESH
NZ, NY, NC, NX = 8, 4, 2, 4
ROWS = 160
TOKS = NY * ROWS
HEAD = 128
COLS = 2 * TOKS
TILE = 256
KINDS = 4
LOW = -1e30
EXP_SCALE = 64 ** (-0.5) * math.log2(math.e)


def rcopy(src, dst, send_sem, recv_sem, device):
    return pltpu.make_async_remote_copy(
        src_ref=src, dst_ref=dst, send_sem=send_sem, recv_sem=recv_sem, device_id=device, device_id_type=MESH
    )


def attention_kernel(
    tok, wq, wk, wv, wo, lam, gain, out,
    xbuf, wloc, wkv, wqs, kv, qrow, qbd, acc, top, wt, hrow, hbuf, osum,
    into, send, tok_r, wy_r, wkv_r, wqs_r, wo_r, w_sib, kv_r, kv_sib, o2_r, o3_r, oc_r, h_r,
):
    z, y, c, x = (lax.axis_index(name) for name in ("z", "y", "core", "x"))
    right, left, facing = lax.rem(x + 1, NX), lax.rem(x + NX - 1, NX), lax.rem(x + 2, NX)
    above, below = lax.rem(y + 1, NY), lax.rem(y + NY - 1, NY)
    across = lax.rem(y + 2, NY)

    inputs = [
        pltpu.make_async_copy(src, dst, into.at[n])
        for n, (src, dst) in enumerate(
            [(wk, wloc.at[1]), (wv, wloc.at[2]), (wq, wloc.at[0]), (tok, xbuf.at[y]), (wo, wt.at[x, z, y, c])]
        )
    ]
    for copy in inputs:
        copy.start()

    barrier = pltpu.get_barrier_semaphore()
    friends = [{"y": lax.rem(y + k, NY)} for k in range(1, NY)]
    friends += [{"z": lax.rem(z + k, NZ)} for k in range(1, NZ)]
    friends += [{"y": lax.rem(y + k, NY), "x": to} for k in range(NY) for to in (left, right)]
    friends += [{"x": facing}, {"core": 1 - c}]
    for friend in friends:
        pl.semaphore_signal(barrier, inc=1, device_id=friend, device_id_type=MESH)
    for copy in inputs:
        copy.wait()
    pl.semaphore_wait(barrier, len(friends))

    half = ROWS // 2

    SEND_TOK, SEND_WY, SEND_W, SEND_KV, SEND_O, SEND_SHARE, SEND_H = range(7)

    def wide(rows):
        return kv.at[pl.ds(0, rows), :]

    def got(sem, ref):
        rcopy(ref, ref, send.at[0], sem, {"core": 1 - c}).wait_recv()

    def gone(group, ref):
        rcopy(ref, ref, send.at[group], oc_r.at[0], {"core": 1 - c}).wait_send()

    share_of = xbuf.shape[2] // 4
    near = pl.ds(pl.multiple_of(lax.rem(x, 2) * share_of, share_of), 3 * share_of)
    missed = pl.ds(pl.multiple_of(lax.rem(x, 2) * 3 * share_of, share_of), share_of)

    def part(slot, k, lanes=near):
        return xbuf.at[slot, pl.ds(k * half, half), lanes]

    def tok_copy(slot, k, n, to):
        rcopy(part(slot, k), part(slot, k), send.at[SEND_TOK], tok_r.at[n], {"y": to}).start()

    def tok_aside(slot, k, n):
        ref = part(slot, k, missed)
        rcopy(ref, ref, send.at[SEND_TOK], tok_r.at[n], {"x": (right, left)[k]}).start()

    def tok_complete(slot, n):
        got(tok_r.at[n], xbuf.at[slot, :, pl.ds(0, share_of)])

    def w_slot(frm, n):
        return (wqs.at[z, frm, c], wkv.at[z, frm, c, :, pl.ds(0, HEAD)], wkv.at[z, frm, c, :, pl.ds(HEAD, HEAD)])[n]

    for n in (1, 2, 0):
        for k in range(1, NY):
            to = lax.rem(y + k, NY)
            src = wloc.at[n, :, pl.ds(pl.multiple_of(to * HEAD, HEAD), HEAD)]
            rcopy(src, w_slot(y, n), send.at[SEND_WY], wy_r.at[min(n, 1)], {"y": to}).start()
    tok_copy(y, 0, 0, above)
    tok_copy(y, 1, 1, below)
    tok_copy(y, 1, 2, above)
    tok_copy(y, 0, 3, below)

    depth = wo.shape[1] // 2
    places = {"y": (y, above, below), "x": (x, right, left)}

    def axes(h):
        return ("y", "x") if h == 0 else ("x", "y")

    def piece(h, a, b, core, z_half=None):
        xx, yy = (b, a) if h == 0 else (a, b)
        zs = slice(None) if z_half is None else pl.ds(z_half * (NZ // 2), NZ // 2)
        return wt.at[xx, zs, yy, core, :, pl.ds(h * depth, depth)]

    def turn(i, at=y):
        return lax.rem(at + jnp.where(i == 2, 3, jnp.where(i == 3, 2, i)), NY)

    def o_second(h, k):
        a, b = (places[name][0] for name in axes(h))
        ref = piece(h, a, b, c)
        to = {axes(h)[0]: lax.rem(a + k, NY)}
        rcopy(ref, ref, send.at[SEND_O], o2_r.at[h, k - 1], to).start()

    def o_share(h, a, b):
        ref = piece(h, a, b, c)
        rcopy(ref, ref, send.at[SEND_SHARE], oc_r.at[0], {"core": 1 - c}).start()

    def o_a(h, i):
        return lax.rem(places[axes(h)[0]][0] + (0, 3, 1, 2)[i], NY)

    def o_third(h, i):
        name = axes(h)[1]
        b, up, down = places[name]
        for k, to, group in [(0, up, 0), (1, down, 0), (1, up, 1), (0, down, 1)]:
            ref = piece(h, o_a(h, i), b, c, k)
            rcopy(ref, ref, send.at[SEND_O], o3_r.at[i, group], {name: to}).start()
        o_share(h, o_a(h, i), b)

    def o_relay(i):
        got(o3_r.at[i, 0], wide(512))
        for h in (1, 0):
            name = axes(h)[1]
            b, up, down = places[name]
            for k, (frm, to) in enumerate(((down, up), (up, down))):
                ref = piece(h, o_a(h, i), frm, c, k)
                rcopy(ref, ref, send.at[SEND_O], o3_r.at[i, 2], {name: to}).start()
        got(o3_r.at[i, 1], wide(512))
        for h in (1, 0):
            for frm in places[axes(h)[1]][1:]:
                o_share(h, o_a(h, i), frm)

    def o_last(i):
        got(o3_r.at[i, 2], wide(512))
        for h in (1, 0):
            o_share(h, o_a(h, i), lax.rem(places[axes(h)[1]][0] + 2, NY))

    def origin(way, d):
        return lax.rem(z + (NZ - d if way == 0 else d), NZ)

    def z_copy(ref, way, reach, group, sem):
        to = lax.rem(z + (reach if way == 0 else NZ - reach), NZ)
        rcopy(ref, ref, send.at[group], sem, {"z": to}).start()

    def share(ref, group, sem):
        rcopy(ref, ref, send.at[group], sem, {"core": 1 - c}).start()

    class Weights:
        def __init__(self, block, sem, sib):
            self.block, self.sem, self.sib = block, sem, sib

        def begin(self):
            for d in (2, 1):
                for kind in (0, 1):
                    for way in (0, 1):
                        z_copy(self.block(z, kind), way, d, SEND_W, self.sem(way, d, kind))
            self.to_sibling(z, (0, 1))

        def to_sibling(self, o, kinds):
            if self.sib is not None:
                for kind in kinds:
                    share(self.block(o, kind), SEND_W, self.sib)

        def pass_on(self, way, kinds):
            o = origin(way, 2)
            for kind in kinds:
                z_copy(self.block(o, kind), way, 1, SEND_W, self.sem(way, 3, kind))
                if way == kind:
                    z_copy(self.block(o, kind), way, 2, SEND_W, self.sem(way, 4, kind))
            self.to_sibling(o, kinds)

        def arrived(self, d):
            for way in (0, 1):
                self.to_sibling(origin(way, d), (0, 1) if d < 4 else (way,))

    key_value = Weights(
        lambda o, kind: wkv.at[o, pl.ds(2 * kind, 2), c],
        lambda way, d, kind: wkv_r.at[2 * way + kind if d == 2 else {1: 4, 4: 5, 3: 6}[d]],
        w_sib.at[0],
    )
    query = Weights(
        lambda o, kind: wqs.at[o, pl.ds(2 * kind, 2), c],
        lambda way, d, kind: wqs_r.at[way if d == 2 else 2],
        w_sib.at[1],
    )
    output = Weights(
        lambda o, kind: wt.at[x, o, y, c, :, pl.ds(kind * depth, depth)], lambda way, d, kind: wo_r.at[way if d == 2 else 2], None
    )

    def kv_block(o, cc, kind):
        return kv.at[pl.ds(pl.multiple_of(((o * NC + cc) * KINDS + kind) * ROWS, ROWS), ROWS), :]

    def farthest(way, kind):
        return NZ // 2 - (way != kind % 2)

    def kv_begin(kind):
        for way in (0, 1):
            z_copy(kv_block(z, c, kind), way, 1, SEND_KV, kv_r.at[way, 0, kind])
        share(kv_block(z, c, kind), SEND_KV, kv_sib.at[z])

    def kv_pass(way, d, kind):
        o = origin(way, d)
        got(kv_r.at[way, d - 1, kind], wide(ROWS))

        @pl.when(d < farthest(way, kind))
        def _():
            z_copy(kv_block(o, c, kind), way, 1, SEND_KV, kv_r.at[way, d, kind])

        share(kv_block(o, c, kind), SEND_KV, kv_sib.at[o])

    output.begin()

    mine = pl.ds(pl.multiple_of(y * HEAD, HEAD), HEAD)
    wqs[z, y, c] = wloc[0, :, mine]
    wkv[z, y, c, :, :HEAD] = wloc[1, :, mine]
    wkv[z, y, c, :, HEAD:] = wloc[2, :, mine]
    acc[...] = jnp.zeros_like(acc)
    top[...] = jnp.full_like(top, LOW)

    got(wy_r.at[1], wide(3 * 32))
    key_value.begin()
    for kind in (0, 1):
        for way in (0, 1):
            got(wkv_r.at[2 * way + kind], wide(64))
            key_value.pass_on(way, (kind,))
    for way in (0, 1):
        got(wo_r.at[way], wide(64))
        output.pass_on(way, (0, 1))
    got(wy_r.at[0], qrow.at[pl.ds(0, 3 * 32), :])
    query.begin()
    got(wkv_r.at[4], wide(256))
    key_value.arrived(1)
    got(tok_r.at[0], part(below, 0))
    tok_copy(below, 0, 4, above)
    tok_aside(below, 0, 6)
    got(tok_r.at[1], part(above, 1))
    tok_copy(above, 1, 4, below)
    tok_aside(above, 1, 5)
    got(wkv_r.at[6], wide(256))
    key_value.arrived(3)
    got(wkv_r.at[5], wide(128))
    key_value.arrived(4)
    for way in (0, 1):
        got(wqs_r.at[way], wide(64))
        query.pass_on(way, (0, 1))
    got(tok_r.at[2], part(below, 1))
    tok_aside(below, 1, 6)
    got(tok_r.at[3], part(above, 0))
    tok_aside(above, 0, 5)
    got(w_sib.at[0], wide(NZ * NY * 32))

    def project(i):
        kv_block(z, c, i)[...] = jnp.dot(
            xbuf[turn(i)], wkv[...].reshape(-1, 2 * HEAD), preferred_element_type=jnp.float32
        ).astype(jnp.bfloat16)
        kv_begin(i)

    def project_near(i, carry):
        @pl.when(i == 1)
        def _():
            tok_complete(above, 5)

        @pl.when(i == 2)
        def _():
            tok_complete(below, 6)

        project(i)
        return carry

    lax.fori_loop(0, NY - 1, project_near, 0)

    got(tok_r.at[4], xbuf.at[across, :, near])
    for k in (0, 1):
        tok_aside(across, k, 7)
    got(wo_r.at[2], wide(10 * 32))
    for h in (1, 0):
        for k in (1, 3, 2):
            o_second(h, k)
        o_third(h, 0)
    got(wqs_r.at[2], wide(10 * 32))
    for d in (1, 3, 4):
        query.arrived(d)
    gone(SEND_WY, qrow.at[pl.ds(0, 9 * 32), :])
    gone(SEND_W, wide(30 * 64 + 30 * 32 + 14 * 32))
    tok_complete(across, 7)
    project(NY - 1)
    for kind in range(NY - 1):
        for way in (0, 1):
            kv_pass(way, 1, kind)
    got(w_sib.at[1], wide(NZ * NY * 16))

    def queries(i, carry):
        at = pl.ds(pl.multiple_of(i * ROWS, ROWS), ROWS)
        qrow[at, :] = jnp.dot(
            xbuf[turn(i)], wqs[...].reshape(-1, HEAD), preferred_element_type=jnp.float32
        ).astype(jnp.bfloat16)
        return carry

    lax.fori_loop(0, NY, queries, 0)
    q_t = qrow[...].T
    first = lax.broadcasted_iota(jnp.int32, q_t.shape, 0) < HEAD // 2
    zero = jnp.zeros_like(q_t)
    qbd[:, :TOKS] = jnp.where(first, q_t, zero)
    qbd[:, TOKS:] = jnp.where(first, zero, q_t)

    ones = jnp.ones((16, NC * TOKS), jnp.bfloat16)

    def place(r, core):
        i = sum((r >= k * ROWS).astype(jnp.int32) for k in range(1, NY))
        return r + ROWS * (2 * turn(i) - i + core)

    def visit(o, masked):
        at = pl.ds(pl.multiple_of(o * NC * TOKS, NC * TOKS), NC * TOKS)
        keys = kv[at, :HEAD]
        values = jnp.concatenate([kv[at, HEAD:].T, ones], axis=0)

        def scores(j):
            return jnp.dot(keys, qbd[:, j * TILE : (j + 1) * TILE], preferred_element_type=jnp.float32)

        ahead = scores(0)
        for j in range(COLS // TILE):
            cols = slice(j * TILE, (j + 1) * TILE)
            s = ahead
            if j + 1 < COLS // TILE:
                ahead = scores(j + 1)
            if masked:
                u = lax.broadcasted_iota(jnp.int32, (NC * TOKS, 1), 0)
                core = (u >= TOKS).astype(jnp.int32)
                t = lax.broadcasted_iota(jnp.int32, (1, TILE), 1) + j * TILE
                t = jnp.where(t >= TOKS, t - TOKS, t)
                s = jnp.where(place(u - TOKS * core, core) <= place(t, c), s, LOW)
            before = top[0:1, cols]
            now = jnp.maximum(before, jnp.max(s, axis=0, keepdims=True))
            shrink = jnp.exp2((before - now) * EXP_SCALE)
            p = jnp.exp2((s - now) * EXP_SCALE).astype(jnp.bfloat16)
            acc[:, cols] = acc[:, cols] * shrink + jnp.dot(values, p, preferred_element_type=jnp.float32)
            top[0:1, cols] = now

    got(kv_sib.at[z], wide(TOKS))
    visit(z, True)

    def pieces_on(h):
        for i, k in ((1, 1), (2, 3), (3, 2)):
            got(o2_r.at[h, k - 1], wide(256))
            o_third(h, i)

    def step(d, carry):
        for way in (0, 1):
            for kind in (2 * way, 2 * way + 1):
                for course in (0, 1):
                    due = d <= farthest(course, kind)

                    @pl.when(due if kind == KINDS - 1 else due & (d > 1))
                    def _():
                        kv_pass(course, d, kind)

            before = d - 1
            o = origin(way, before)
            there = (before >= 1) & (before <= NZ // 2 - way)

            @pl.when(there)
            def _():
                got(kv_sib.at[o], wide(TOKS))

            @pl.when(there & (o < z))
            def _():
                visit(o, False)

            if way == 0:

                @pl.when(d == 2)
                def _():
                    pieces_on(0)

        @pl.when(d == 1)
        def _():
            pieces_on(1)

        for i, at in enumerate((2, 3, 4, 4)):

            @pl.when(d == at)
            def _():
                o_relay(i)

        return carry

    lax.fori_loop(1, NZ // 2 + 2, step, 0)

    def part_of(cols):
        return acc[:HEAD, cols] / acc[HEAD : HEAD + 1, cols]

    mixture = part_of(slice(0, TOKS)) - lam[y] * part_of(slice(TOKS, COLS))
    scale = lax.rsqrt(jnp.mean(mixture * mixture, axis=0, keepdims=True) + 1e-05)
    hrow[...] = ((mixture * scale).T * gain[...]).astype(jnp.bfloat16).reshape(NY, ROWS, HEAD)

    def rows(k):
        return pl.ds(k * half, half)

    def h_copy(i, k, sem, device):
        dst = hbuf.at[x, rows(k), pl.ds(pl.multiple_of(y * HEAD, HEAD), HEAD)]
        rcopy(hrow.at[i, rows(k), :], dst, send.at[SEND_H], h_r.at[sem], {"y": turn(i), **device}).start()

    for i in range(1, NY):
        for k in (0, 1):
            h_copy(i, k, 0, {})
    for k, to, sem in [(0, right, 1), (1, left, 2), (1, right, 3), (0, left, 3)]:
        for i in range(NY):
            h_copy(i, k, sem, {"x": to})
    hbuf[x, :, mine] = hrow[0]
    for i in range(NY):
        o_last(i)
    for k, (frm, to) in enumerate(((left, right), (right, left))):
        got(h_r.at[1 + k], wide(2 * half))
        ref = hbuf.at[frm, rows(k), :]
        rcopy(ref, ref, send.at[SEND_H], h_r.at[4], {"x": to}).start()
    got(h_r.at[0], wide(3 * half))

    def product(xx):
        return lax.dot_general(
            hbuf[xx],
            wt[xx].reshape(-1, wo.shape[1]),
            (((1,), (1,)), ((), ())),
            preferred_element_type=jnp.float32,
        )

    got(oc_r.at[0], wt.at[pl.ds(0, 2)])
    osum[...] = product(x)
    gone(SEND_O, wide(6 * 256 + 48 * 128))
    gone(SEND_SHARE, wt.at[pl.ds(0, 2)])
    gone(SEND_TOK, xbuf.at[pl.ds(0, 3)])
    gone(SEND_KV, wide(60 * ROWS))
    got(h_r.at[3], wide(4 * half))
    osum[...] += product(left) + product(right)
    got(h_r.at[4], wide(4 * half))
    out[...] = (osum[...] + product(facing)).astype(jnp.bfloat16)

    gone(SEND_H, wide(22 * half // 2 + 4 * half))


def attention(tokens, wq, wk, wv, wo, lam, gain):
    vmem = pl.BlockSpec(memory_space=pltpu.VMEM)
    hbm = pl.BlockSpec(memory_space=pltpu.HBM)
    dma = pltpu.SemaphoreType.DMA
    width = tokens.shape[1]
    return pl.pallas_call(
        attention_kernel,
        out_shape=jax.ShapeDtypeStruct(tokens.shape, jnp.bfloat16),
        in_specs=[hbm, hbm, hbm, hbm, hbm, pl.BlockSpec(memory_space=pltpu.SMEM), vmem],
        out_specs=vmem,
        scratch_shapes=[
            pltpu.VMEM((NY, ROWS, width), jnp.bfloat16),
            pltpu.VMEM((3, *wq.shape), jnp.bfloat16),
            pltpu.VMEM((NZ, NY, NC, wq.shape[0], 2 * HEAD), jnp.bfloat16),
            pltpu.VMEM((NZ, NY, NC, wq.shape[0], HEAD), jnp.bfloat16),
            pltpu.VMEM((NZ * NC * TOKS, 2 * HEAD), jnp.bfloat16),
            pltpu.VMEM((TOKS, HEAD), jnp.bfloat16),
            pltpu.VMEM((HEAD, COLS), jnp.bfloat16),
            pltpu.VMEM((HEAD + 16, COLS), jnp.float32),
            pltpu.VMEM((8, COLS), jnp.float32),
            pltpu.VMEM((NX, NZ, NY, NC, wo.shape[0], wo.shape[1]), jnp.bfloat16),
            pltpu.VMEM((NY, ROWS, HEAD), jnp.bfloat16),
            pltpu.VMEM((NX, ROWS, NY * HEAD), jnp.bfloat16),
            pltpu.VMEM((ROWS, width), jnp.float32),
            dma((5,)),
            dma((7,)),
            dma((8,)),
            dma((2,)),
            dma((7,)),
            dma((3,)),
            dma((3,)),
            dma((2,)),
            dma((2, NZ // 2, KINDS)),
            dma((NZ,)),
            dma((2, NY - 1)),
            dma((NY, 3)),
            dma((1,)),
            dma((5,)),
        ],
        compiler_params=pltpu.CompilerParams(
            collective_id=0, has_side_effects=True, vmem_limit_bytes=56 * 1024 * 1024
        ),
        name="attention",
    )(tokens, wq, wk, wv, wo, lam, gain.reshape(1, -1))


def on_device(tokens, query_weight, key_weight, value_weight, out_weight, mix_lambda, head_gain):
    return attention(tokens, query_weight, key_weight, value_weight, out_weight.T, mix_lambda, head_gain)


def solution(mesh):
    fine = Mesh(mesh.devices.reshape(NZ, NY, NC, NX), ("z", "y", "core", "x"))
    sp = ("z", "y", "core")
    placed = (P(sp, None), P(sp, "x"), P(sp, "x"), P(sp, "x"), P("x", sp), P("x"), P())
    return jax.shard_map(on_device, mesh=fine, in_specs=placed, out_specs=P(sp, None), check_vma=False)
```

```python
import functools
import math

import jax
import jax.numpy as jnp
from jax import lax
from jax.experimental import pallas as pl
from jax.experimental.pallas import tpu as pltpu
from jax.sharding import Mesh
from jax.sharding import PartitionSpec as P

MESH = pl.DeviceIdType.MESH
NZ, NY, NC, NX = 8, 4, 2, 4
ROWS = 160
TOKS = NY * ROWS
HEAD = 128
COLS = 2 * TOKS
TILE = 256
KINDS = 4
LOW = -1e30
EXP_SCALE = 64 ** (-0.5) * math.log2(math.e)


def rcopy(src, dst, send_sem, recv_sem, device):
    return pltpu.make_async_remote_copy(
        src_ref=src, dst_ref=dst, send_sem=send_sem, recv_sem=recv_sem, device_id=device, device_id_type=MESH
    )


def attention_kernel(
    tok, wq, wk, wv, wo, lam, gain, out,
    xbuf, wloc, wkv, wqs, kv, qrow, qbd, acc, top, wt, hrow, hbuf, osum,
    into, send, tok_r, wy_r, wkv_r, wqs_r, wo_r, w_sib, kv_r, kv_sib, o2_r, o3_r, oc_r, h_r,
):
    z, y, c, x = (lax.axis_index(name) for name in ("z", "y", "core", "x"))
    right, left, facing = lax.rem(x + 1, NX), lax.rem(x + NX - 1, NX), lax.rem(x + 2, NX)
    above, below = lax.rem(y + 1, NY), lax.rem(y + NY - 1, NY)
    across = lax.rem(y + 2, NY)

    inputs = [
        pltpu.make_async_copy(src, dst, into.at[n])
        for n, (src, dst) in enumerate(
            [(wk, wloc.at[1]), (wv, wloc.at[2]), (wq, wloc.at[0]), (tok, xbuf.at[y]), (wo, wt.at[x, z, y, c])]
        )
    ]
    for copy in inputs:
        copy.start()

    barrier = pltpu.get_barrier_semaphore()
    friends = [{"y": lax.rem(y + k, NY)} for k in range(1, NY)]
    friends += [{"z": lax.rem(z + k, NZ)} for k in range(1, NZ)]
    friends += [{"y": lax.rem(y + k, NY), "x": to} for k in range(NY) for to in (left, right)]
    friends += [{"x": facing}, {"core": 1 - c}]
    for friend in friends:
        pl.semaphore_signal(barrier, inc=1, device_id=friend, device_id_type=MESH)
    for copy in inputs:
        copy.wait()
    pl.semaphore_wait(barrier, len(friends))

    half = ROWS // 2

    SEND_TOK, SEND_WY, SEND_W, SEND_KV, SEND_O, SEND_SHARE, SEND_H = range(7)

    def wide(rows):
        return kv.at[pl.ds(0, rows), :]

    def got(sem, ref):
        rcopy(ref, ref, send.at[0], sem, {"core": 1 - c}).wait_recv()

    def gone(group, ref):
        rcopy(ref, ref, send.at[group], oc_r.at[0], {"core": 1 - c}).wait_send()

    share_of = xbuf.shape[2] // 4
    near = pl.ds(pl.multiple_of(lax.rem(x, 2) * share_of, share_of), 3 * share_of)
    missed = pl.ds(pl.multiple_of(lax.rem(x, 2) * 3 * share_of, share_of), share_of)

    def part(slot, k, lanes=near):
        return xbuf.at[slot, pl.ds(k * half, half), lanes]

    def tok_copy(slot, k, n, to):
        rcopy(part(slot, k), part(slot, k), send.at[SEND_TOK], tok_r.at[n], {"y": to}).start()

    def tok_aside(slot, k, n):
        ref = part(slot, k, missed)
        rcopy(ref, ref, send.at[SEND_TOK], tok_r.at[n], {"x": (right, left)[k]}).start()

    def tok_complete(slot, n):
        got(tok_r.at[n], xbuf.at[slot, :, pl.ds(0, share_of)])

    def w_slot(frm, n):
        return (wqs.at[z, frm, c], wkv.at[z, frm, c, :, pl.ds(0, HEAD)], wkv.at[z, frm, c, :, pl.ds(HEAD, HEAD)])[n]

    for n in (1, 2, 0):
        for k in range(1, NY):
            to = lax.rem(y + k, NY)
            src = wloc.at[n, :, pl.ds(pl.multiple_of(to * HEAD, HEAD), HEAD)]
            rcopy(src, w_slot(y, n), send.at[SEND_WY], wy_r.at[min(n, 1)], {"y": to}).start()
    tok_copy(y, 0, 0, above)
    tok_copy(y, 1, 1, below)
    tok_copy(y, 1, 2, above)
    tok_copy(y, 0, 3, below)

    depth = wo.shape[1] // 2
    places = {"y": (y, above, below), "x": (x, right, left)}

    def axes(h):
        return ("y", "x") if h == 0 else ("x", "y")

    def piece(h, a, b, core, z_half=None):
        xx, yy = (b, a) if h == 0 else (a, b)
        zs = slice(None) if z_half is None else pl.ds(z_half * (NZ // 2), NZ // 2)
        return wt.at[xx, zs, yy, core, :, pl.ds(h * depth, depth)]

    def turn(i, at=y):
        return lax.rem(at + jnp.where(i == 2, 3, jnp.where(i == 3, 2, i)), NY)

    def o_second(h, k):
        a, b = (places[name][0] for name in axes(h))
        ref = piece(h, a, b, c)
        to = {axes(h)[0]: lax.rem(a + k, NY)}
        rcopy(ref, ref, send.at[SEND_O], o2_r.at[h, k - 1], to).start()

    def o_share(h, a, b):
        ref = piece(h, a, b, c)
        rcopy(ref, ref, send.at[SEND_SHARE], oc_r.at[0], {"core": 1 - c}).start()

    def o_a(h, i):
        return lax.rem(places[axes(h)[0]][0] + (0, 3, 1, 2)[i], NY)

    def o_third(h, i):
        name = axes(h)[1]
        b, up, down = places[name]
        for k, to, group in [(0, up, 0), (1, down, 0), (1, up, 1), (0, down, 1)]:
            ref = piece(h, o_a(h, i), b, c, k)
            rcopy(ref, ref, send.at[SEND_O], o3_r.at[i, group], {name: to}).start()
        o_share(h, o_a(h, i), b)

    def o_relay(i):
        got(o3_r.at[i, 0], wide(512))
        for h in (1, 0):
            name = axes(h)[1]
            b, up, down = places[name]
            for k, (frm, to) in enumerate(((down, up), (up, down))):
                ref = piece(h, o_a(h, i), frm, c, k)
                rcopy(ref, ref, send.at[SEND_O], o3_r.at[i, 2], {name: to}).start()
        got(o3_r.at[i, 1], wide(512))
        for h in (1, 0):
            for frm in places[axes(h)[1]][1:]:
                o_share(h, o_a(h, i), frm)

    def o_last(i):
        got(o3_r.at[i, 2], wide(512))
        for h in (1, 0):
            o_share(h, o_a(h, i), lax.rem(places[axes(h)[1]][0] + 2, NY))

    def origin(way, d):
        return lax.rem(z + (NZ - d if way == 0 else d), NZ)

    def z_copy(ref, way, reach, group, sem):
        to = lax.rem(z + (reach if way == 0 else NZ - reach), NZ)
        rcopy(ref, ref, send.at[group], sem, {"z": to}).start()

    def share(ref, group, sem):
        rcopy(ref, ref, send.at[group], sem, {"core": 1 - c}).start()

    class Weights:
        def __init__(self, block, sem, sib):
            self.block, self.sem, self.sib = block, sem, sib

        def begin(self):
            for d in (2, 1):
                for kind in (0, 1):
                    for way in (0, 1):
                        z_copy(self.block(z, kind), way, d, SEND_W, self.sem(way, d, kind))
            self.to_sibling(z, (0, 1))

        def to_sibling(self, o, kinds):
            if self.sib is not None:
                for kind in kinds:
                    share(self.block(o, kind), SEND_W, self.sib)

        def pass_on(self, way, kinds):
            o = origin(way, 2)
            for kind in kinds:
                z_copy(self.block(o, kind), way, 1, SEND_W, self.sem(way, 3, kind))
                if way == kind:
                    z_copy(self.block(o, kind), way, 2, SEND_W, self.sem(way, 4, kind))
            self.to_sibling(o, kinds)

        def arrived(self, d):
            for way in (0, 1):
                self.to_sibling(origin(way, d), (0, 1) if d < 4 else (way,))

    key_value = Weights(
        lambda o, kind: wkv.at[o, pl.ds(2 * kind, 2), c],
        lambda way, d, kind: wkv_r.at[2 * way + kind if d == 2 else {1: 4, 4: 5, 3: 6}[d]],
        w_sib.at[0],
    )
    query = Weights(
        lambda o, kind: wqs.at[o, pl.ds(2 * kind, 2), c],
        lambda way, d, kind: wqs_r.at[way if d == 2 else 2],
        w_sib.at[1],
    )
    output = Weights(
        lambda o, kind: wt.at[x, o, y, c, :, pl.ds(kind * depth, depth)], lambda way, d, kind: wo_r.at[way if d == 2 else 2], None
    )

    def kv_block(o, cc, kind):
        return kv.at[pl.ds(pl.multiple_of(((o * NC + cc) * KINDS + kind) * ROWS, ROWS), ROWS), :]

    def farthest(way, kind):
        return NZ // 2 - (way != kind % 2)

    def kv_begin(kind):
        for way in (0, 1):
            z_copy(kv_block(z, c, kind), way, 1, SEND_KV, kv_r.at[way, 0, kind])
        share(kv_block(z, c, kind), SEND_KV, kv_sib.at[z])

    def kv_pass(way, d, kind):
        o = origin(way, d)
        got(kv_r.at[way, d - 1, kind], wide(ROWS))

        @pl.when(d < farthest(way, kind))
        def _():
            z_copy(kv_block(o, c, kind), way, 1, SEND_KV, kv_r.at[way, d, kind])

        share(kv_block(o, c, kind), SEND_KV, kv_sib.at[o])

    output.begin()

    mine = pl.ds(pl.multiple_of(y * HEAD, HEAD), HEAD)
    wqs[z, y, c] = wloc[0, :, mine]
    wkv[z, y, c, :, :HEAD] = wloc[1, :, mine]
    wkv[z, y, c, :, HEAD:] = wloc[2, :, mine]
    acc[...] = jnp.zeros_like(acc)
    top[...] = jnp.full_like(top, LOW)

    got(wy_r.at[1], wide(3 * 32))
    key_value.begin()
    for kind in (0, 1):
        for way in (0, 1):
            got(wkv_r.at[2 * way + kind], wide(64))
            key_value.pass_on(way, (kind,))
    for way in (0, 1):
        got(wo_r.at[way], wide(64))
        output.pass_on(way, (0, 1))
    got(wy_r.at[0], qrow.at[pl.ds(0, 3 * 32), :])
    query.begin()
    got(wkv_r.at[4], wide(256))
    key_value.arrived(1)
    got(tok_r.at[0], part(below, 0))
    tok_copy(below, 0, 4, above)
    tok_aside(below, 0, 6)
    got(tok_r.at[1], part(above, 1))
    tok_copy(above, 1, 4, below)
    tok_aside(above, 1, 5)
    got(wkv_r.at[6], wide(256))
    key_value.arrived(3)
    got(wkv_r.at[5], wide(128))
    key_value.arrived(4)
    for way in (0, 1):
        got(wqs_r.at[way], wide(64))
        query.pass_on(way, (0, 1))
    got(tok_r.at[2], part(below, 1))
    tok_aside(below, 1, 6)
    got(tok_r.at[3], part(above, 0))
    tok_aside(above, 0, 5)
    got(w_sib.at[0], wide(NZ * NY * 32))

    def project(i):
        kv_block(z, c, i)[...] = jnp.dot(
            xbuf[turn(i)], wkv[...].reshape(-1, 2 * HEAD), preferred_element_type=jnp.float32
        ).astype(jnp.bfloat16)
        kv_begin(i)

    def project_near(i, carry):
        @pl.when(i == 1)
        def _():
            tok_complete(above, 5)

        @pl.when(i == 2)
        def _():
            tok_complete(below, 6)

        project(i)
        return carry

    lax.fori_loop(0, NY - 1, project_near, 0)

    got(tok_r.at[4], xbuf.at[across, :, near])
    for k in (0, 1):
        tok_aside(across, k, 7)
    got(wo_r.at[2], wide(10 * 32))
    for h in (1, 0):
        for k in (1, 3, 2):
            o_second(h, k)
        o_third(h, 0)
    got(wqs_r.at[2], wide(10 * 32))
    for d in (1, 3, 4):
        query.arrived(d)
    gone(SEND_WY, qrow.at[pl.ds(0, 9 * 32), :])
    gone(SEND_W, wide(30 * 64 + 30 * 32 + 14 * 32))
    for way in (0, 1):
        kv_pass(way, 1, 0)
    tok_complete(across, 7)
    project(NY - 1)
    for kind in range(1, NY - 1):
        for way in (0, 1):
            kv_pass(way, 1, kind)
    got(w_sib.at[1], wide(NZ * NY * 16))

    def queries(i, carry):
        at = pl.ds(pl.multiple_of(i * ROWS, ROWS), ROWS)
        qrow[at, :] = jnp.dot(
            xbuf[turn(i)], wqs[...].reshape(-1, HEAD), preferred_element_type=jnp.float32
        ).astype(jnp.bfloat16)
        return carry

    lax.fori_loop(0, NY, queries, 0)
    q_t = qrow[...].T
    first = lax.broadcasted_iota(jnp.int32, q_t.shape, 0) < HEAD // 2
    zero = jnp.zeros_like(q_t)
    qbd[:, :TOKS] = jnp.where(first, q_t, zero)
    qbd[:, TOKS:] = jnp.where(first, zero, q_t)

    ones = jnp.ones((16, NC * TOKS), jnp.bfloat16)

    def place(r, core):
        i = sum((r >= k * ROWS).astype(jnp.int32) for k in range(1, NY))
        return r + ROWS * (2 * turn(i) - i + core)

    def visit(o, masked):
        at = pl.ds(pl.multiple_of(o * NC * TOKS, NC * TOKS), NC * TOKS)
        keys = kv[at, :HEAD]
        values = jnp.concatenate([kv[at, HEAD:].T, ones], axis=0)

        def scores(j):
            return jnp.dot(keys, qbd[:, j * TILE : (j + 1) * TILE], preferred_element_type=jnp.float32)

        ahead = scores(0)
        for j in range(COLS // TILE):
            cols = slice(j * TILE, (j + 1) * TILE)
            s = ahead
            if j + 1 < COLS // TILE:
                ahead = scores(j + 1)
            if masked:
                u = lax.broadcasted_iota(jnp.int32, (NC * TOKS, 1), 0)
                core = (u >= TOKS).astype(jnp.int32)
                t = lax.broadcasted_iota(jnp.int32, (1, TILE), 1) + j * TILE
                t = jnp.where(t >= TOKS, t - TOKS, t)
                s = jnp.where(place(u - TOKS * core, core) <= place(t, c), s, LOW)
            before = top[0:1, cols]
            now = jnp.maximum(before, jnp.max(s, axis=0, keepdims=True))
            shrink = jnp.exp2((before - now) * EXP_SCALE)
            p = jnp.exp2((s - now) * EXP_SCALE).astype(jnp.bfloat16)
            acc[:, cols] = acc[:, cols] * shrink + jnp.dot(values, p, preferred_element_type=jnp.float32)
            top[0:1, cols] = now

    got(kv_sib.at[z], wide(TOKS))
    visit(z, True)

    def pieces_on(h):
        for i, k in ((1, 1), (2, 3), (3, 2)):
            got(o2_r.at[h, k - 1], wide(256))
            o_third(h, i)

    def step(d, carry):
        for way in (0, 1):
            for kind in (2 * way, 2 * way + 1):
                for course in (0, 1):
                    due = d <= farthest(course, kind)

                    @pl.when(due if kind == KINDS - 1 else due & (d > 1))
                    def _():
                        kv_pass(course, d, kind)

            before = d - 1
            o = origin(way, before)
            there = (before >= 1) & (before <= NZ // 2 - way)

            @pl.when(there)
            def _():
                got(kv_sib.at[o], wide(TOKS))

            @pl.when(there & (o < z))
            def _():
                visit(o, False)

            if way == 0:

                @pl.when(d == 2)
                def _():
                    pieces_on(0)

        @pl.when(d == 1)
        def _():
            pieces_on(1)

        for i, at in enumerate((2, 3, 4, 4)):

            @pl.when(d == at)
            def _():
                o_relay(i)

        return carry

    lax.fori_loop(1, NZ // 2 + 2, step, 0)

    def part_of(cols):
        return acc[:HEAD, cols] / acc[HEAD : HEAD + 1, cols]

    mixture = part_of(slice(0, TOKS)) - lam[y] * part_of(slice(TOKS, COLS))
    scale = lax.rsqrt(jnp.mean(mixture * mixture, axis=0, keepdims=True) + 1e-05)
    hrow[...] = ((mixture * scale).T * gain[...]).astype(jnp.bfloat16).reshape(NY, ROWS, HEAD)

    def rows(k):
        return pl.ds(k * half, half)

    def h_copy(i, k, sem, device):
        dst = hbuf.at[x, rows(k), pl.ds(pl.multiple_of(y * HEAD, HEAD), HEAD)]
        rcopy(hrow.at[i, rows(k), :], dst, send.at[SEND_H], h_r.at[sem], {"y": turn(i), **device}).start()

    for i in range(1, NY):
        for k in (0, 1):
            h_copy(i, k, 0, {})
    for k, to, sem in [(0, right, 1), (1, left, 2), (1, right, 3), (0, left, 3)]:
        for i in range(NY):
            h_copy(i, k, sem, {"x": to})
    hbuf[x, :, mine] = hrow[0]
    for i in range(NY):
        o_last(i)
    for k, (frm, to) in enumerate(((left, right), (right, left))):
        got(h_r.at[1 + k], wide(2 * half))
        ref = hbuf.at[frm, rows(k), :]
        rcopy(ref, ref, send.at[SEND_H], h_r.at[4], {"x": to}).start()
    got(h_r.at[0], wide(3 * half))

    def product(xx):
        return lax.dot_general(
            hbuf[xx],
            wt[xx].reshape(-1, wo.shape[1]),
            (((1,), (1,)), ((), ())),
            preferred_element_type=jnp.float32,
        )

    got(oc_r.at[0], wt.at[pl.ds(0, 2)])
    osum[...] = product(x)
    gone(SEND_O, wide(6 * 256 + 48 * 128))
    gone(SEND_SHARE, wt.at[pl.ds(0, 2)])
    gone(SEND_TOK, xbuf.at[pl.ds(0, 3)])
    gone(SEND_KV, wide(60 * ROWS))
    got(h_r.at[3], wide(4 * half))
    osum[...] += product(left) + product(right)
    got(h_r.at[4], wide(4 * half))
    out[...] = (osum[...] + product(facing)).astype(jnp.bfloat16)

    gone(SEND_H, wide(22 * half // 2 + 4 * half))


def attention(tokens, wq, wk, wv, wo, lam, gain):
    vmem = pl.BlockSpec(memory_space=pltpu.VMEM)
    hbm = pl.BlockSpec(memory_space=pltpu.HBM)
    dma = pltpu.SemaphoreType.DMA
    width = tokens.shape[1]
    return pl.pallas_call(
        attention_kernel,
        out_shape=jax.ShapeDtypeStruct(tokens.shape, jnp.bfloat16),
        in_specs=[hbm, hbm, hbm, hbm, hbm, pl.BlockSpec(memory_space=pltpu.SMEM), vmem],
        out_specs=vmem,
        scratch_shapes=[
            pltpu.VMEM((NY, ROWS, width), jnp.bfloat16),
            pltpu.VMEM((3, *wq.shape), jnp.bfloat16),
            pltpu.VMEM((NZ, NY, NC, wq.shape[0], 2 * HEAD), jnp.bfloat16),
            pltpu.VMEM((NZ, NY, NC, wq.shape[0], HEAD), jnp.bfloat16),
            pltpu.VMEM((NZ * NC * TOKS, 2 * HEAD), jnp.bfloat16),
            pltpu.VMEM((TOKS, HEAD), jnp.bfloat16),
            pltpu.VMEM((HEAD, COLS), jnp.bfloat16),
            pltpu.VMEM((HEAD + 16, COLS), jnp.float32),
            pltpu.VMEM((8, COLS), jnp.float32),
            pltpu.VMEM((NX, NZ, NY, NC, wo.shape[0], wo.shape[1]), jnp.bfloat16),
            pltpu.VMEM((NY, ROWS, HEAD), jnp.bfloat16),
            pltpu.VMEM((NX, ROWS, NY * HEAD), jnp.bfloat16),
            pltpu.VMEM((ROWS, width), jnp.float32),
            dma((5,)),
            dma((7,)),
            dma((8,)),
            dma((2,)),
            dma((7,)),
            dma((3,)),
            dma((3,)),
            dma((2,)),
            dma((2, NZ // 2, KINDS)),
            dma((NZ,)),
            dma((2, NY - 1)),
            dma((NY, 3)),
            dma((1,)),
            dma((5,)),
        ],
        compiler_params=pltpu.CompilerParams(
            collective_id=0, has_side_effects=True, vmem_limit_bytes=56 * 1024 * 1024
        ),
        name="attention",
    )(tokens, wq, wk, wv, wo, lam, gain.reshape(1, -1))


def on_device(tokens, query_weight, key_weight, value_weight, out_weight, mix_lambda, head_gain):
    return attention(tokens, query_weight, key_weight, value_weight, out_weight.T, mix_lambda, head_gain)


def solution(mesh):
    fine = Mesh(mesh.devices.reshape(NZ, NY, NC, NX), ("z", "y", "core", "x"))
    sp = ("z", "y", "core")
    placed = (P(sp, None), P(sp, "x"), P(sp, "x"), P(sp, "x"), P("x", sp), P("x"), P())
    return jax.shard_map(on_device, mesh=fine, in_specs=placed, out_specs=P(sp, None), check_vma=False)
```
